512 devices in a mesh: fs: 64 (over z, y), tp: 8 (over x, core).
Axes of the slice: x: 4, y: 8, z: 8, core: 2. Of those that a mesh axis runs over, the one named last changes fastest.
Arguments:
- x_late: bfloat16 [12288, 2048], P(('fs', 'tp')), may hold values from -6 to 6
- x_early: bfloat16 [12288, 2048], P(('fs', 'tp')), may hold values from -6 to 6
- cotangent: bfloat16 [12288, 2048], P(('fs', 'tp')), may hold values from -1.25 to 1.25
- norm_gain: bfloat16 [2048], replicated, may hold values from 0.099609375 to 1.8984375
- gate_weight: bfloat16 [2048, 2816], P('fs', 'tp'), may hold values from -0.125 to 0.125
- up_weight: bfloat16 [2048, 2816], P('fs', 'tp'), may hold values from -0.125 to 0.125
- down_weight: bfloat16 [2048, 2816], P('fs', 'tp'), may hold values from -0.109375 to 0.109375
- gate_sum: float32 [2048, 2816], P('fs', 'tp'), may hold values from -6 to 6
- up_sum: float32 [2048, 2816], P('fs', 'tp'), may hold values from -6 to 6
- down_sum: float32 [2048, 2816], P('fs', 'tp'), may hold values from -6 to 6
Outputs:
- out_late: bfloat16 [12288, 2048], P(('fs', 'tp'))
- grad_early: bfloat16 [12288, 2048], P(('fs', 'tp'))
- gate_sum_out: float32 [2048, 2816], P('fs', 'tp')
- up_sum_out: float32 [2048, 2816], P('fs', 'tp')
- down_sum_out: float32 [2048, 2816], P('fs', 'tp')
The draws below stay inside these ranges and needn't reach their ends.
All inputs are finite; a program needn't handle non-finite values.
Results may differ from the reference program's by a relative error of at most 0.0095.
Values may be sent and summed in bfloat16 or wider, within the bound.
No kernel may reach another device: no remote copies, remote signals or barrier semaphores. Data moves between devices by JAX's collectives and lax.ppermute only.
A program may use at most 64 MiB of HBM per device.

```python
import jax
import jax.numpy as jnp
from jax import lax

D = 2048
FF = 2816
TOKENS = 12288
N_TP = 8


def strengthened(array, key, source, target, shards_of, factor):
    owner, partner = [(jnp.arange(array.shape[dim]) // (array.shape[dim] // shards_of)).reshape([-1 if axis == dim else 1 for axis in range(array.ndim)]) for dim in (source, target)]
    chosen = jax.random.permutation(key, shards_of)[partner]
    strong = (owner == chosen) | (owner == (partner + shards_of // 2) % shards_of)
    return jnp.where(strong, factor * array, array)


def block_levels(key, dims, pieces, low, top_value):
    def one(axis_at, parts):
        heights = jax.random.uniform(jax.random.fold_in(jax.random.fold_in(key, 6), axis_at), (parts,), jnp.float32, low / len(pieces), top_value / len(pieces))
        return jnp.repeat(jnp.exp(heights), dims[axis_at] // parts).reshape((-1,) + (1,) * (len(dims) - axis_at - 1))

    loudness = one(*pieces[0])
    for cut in pieces[1:]:
        loudness = loudness * one(*cut)
    return loudness


def normal_values(rng, shape, deviation, reach, split=(), dtype=jnp.bfloat16):
    drawn = deviation * jax.random.normal(rng, shape, jnp.float32)
    if split:
        drawn = drawn * block_levels(rng, shape, split, -0.22, 0.18)
    return jnp.clip(drawn, -reach, reach).astype(dtype)


def noise_with(key, dims, scale, limit, pieces, heavy, kind=jnp.bfloat16):
    entries = scale * jax.random.normal(key, dims, jnp.float32)
    if pieces:
        entries = entries * block_levels(key, dims, pieces, -0.22, 0.18)
    return jnp.clip(strengthened(entries, jax.random.fold_in(key, 3), *heavy), -limit, limit).astype(kind)


def setup_inputs(seed: int = 0) -> dict:
    key_of = jax.random.split(jax.random.key(seed), 11)
    x_late = normal_values(key_of[0], (TOKENS, D), 1.0, 6.0, ((0, 512),))
    x_early = normal_values(key_of[1], (TOKENS, D), 1.0, 6.0, ((0, 512),))
    cotangent = noise_with(key_of[2], (TOKENS, D), 0.05, 1.25, ((0, 512),), (0, 1, 512, 6.0))
    norm_gain = jnp.clip(1.0 + 0.18 * jax.random.normal(key_of[3], (D,), jnp.float32), 0.099609375, 1.8984375).astype(jnp.bfloat16)
    gate_weight = normal_values(key_of[4], (D, FF), D ** -0.5, 0.125, ((0, 64), (1, 8)))
    up_weight = normal_values(key_of[5], (D, FF), D ** -0.5, 0.125, ((0, 64), (1, 8)))
    down_weight = normal_values(key_of[6], (D, FF), FF ** -0.5, 0.109375, ((0, 64), (1, 8)))
    gate_sum = normal_values(key_of[7], (D, FF), 1.0, 6.0, ((0, 64), (1, 8)), jnp.float32)
    up_sum = normal_values(key_of[8], (D, FF), 1.0, 6.0, ((0, 64), (1, 8)), jnp.float32)
    down_sum = normal_values(key_of[9], (D, FF), 1.0, 6.0, ((0, 64), (1, 8)), jnp.float32)
    return {"x_late": x_late, "x_early": x_early, "cotangent": cotangent, "norm_gain": norm_gain, "gate_weight": gate_weight, "up_weight": up_weight, "down_weight": down_weight, "gate_sum": gate_sum, "up_sum": up_sum, "down_sum": down_sum}


eps = 1e-06

def normalize(x, norm_gain):
    xf = x.astype(jnp.float32)
    inv = lax.rsqrt(lax.optimization_barrier(jnp.mean(xf * xf, axis=-1, keepdims=True)) + eps)
    return (xf, inv, (xf * inv * norm_gain.astype(jnp.float32)).astype(jnp.bfloat16))

def block_sum(pairs):
    width = FF // N_TP
    total = jnp.zeros((pairs[0][0].shape[0], pairs[0][1].shape[0]), jnp.float32)
    for block in range(N_TP):
        part = jnp.zeros_like(total)
        for left, right in pairs:
            part = part + jnp.dot(left[:, block * width:(block + 1) * width], right[:, block * width:(block + 1) * width].T, preferred_element_type=jnp.float32)
        rounded = lax.optimization_barrier(part.astype(jnp.bfloat16))
        total = total + rounded.astype(jnp.float32)
    return total

def reference(x_late, x_early, cotangent, norm_gain, gate_weight, up_weight, down_weight, gate_sum, up_sum, down_sum):
    late_f, late_inv, normed_late = normalize(x_late, norm_gain)
    gate_l = jnp.dot(normed_late, gate_weight, preferred_element_type=jnp.float32)
    up_l = jnp.dot(normed_late, up_weight, preferred_element_type=jnp.float32)
    hidden_l = (jax.nn.silu(gate_l) * up_l).astype(jnp.bfloat16)
    branch = block_sum([(hidden_l, down_weight)])
    out_late = (late_f + 0.5 * branch).astype(jnp.bfloat16)
    early_f, inv, normed_early = normalize(x_early, norm_gain)
    gate_e = jnp.dot(normed_early, gate_weight, preferred_element_type=jnp.float32)
    up_e = jnp.dot(normed_early, up_weight, preferred_element_type=jnp.float32)
    sig = jax.nn.sigmoid(gate_e)
    silu_e = gate_e * sig
    hidden_e = (silu_e * up_e).astype(jnp.bfloat16)
    half_cot = (0.5 * cotangent.astype(jnp.float32)).astype(jnp.bfloat16)
    down_grad = jnp.dot(half_cot.T, hidden_e, preferred_element_type=jnp.float32)
    d_hidden = jnp.dot(half_cot, down_weight, preferred_element_type=jnp.float32)
    d_gate = (d_hidden * up_e * sig * (1.0 + gate_e * (1.0 - sig))).astype(jnp.bfloat16)
    d_up = (d_hidden * silu_e).astype(jnp.bfloat16)
    gate_grad = jnp.dot(normed_early.T, d_gate, preferred_element_type=jnp.float32)
    up_grad = jnp.dot(normed_early.T, d_up, preferred_element_type=jnp.float32)
    d_normed = block_sum([(d_gate, gate_weight), (d_up, up_weight)])
    scaled = d_normed * norm_gain.astype(jnp.float32)
    d_input = inv * scaled - early_f * inv ** 3 * lax.optimization_barrier(jnp.mean(scaled * early_f, axis=-1, keepdims=True))
    grad_early = (cotangent.astype(jnp.float32) + d_input).astype(jnp.bfloat16)
    return (out_late, grad_early, gate_sum + gate_grad, up_sum + up_grad, down_sum + down_grad)
```

```python
import functools

import jax
import jax.numpy as jnp
from jax import lax
from jax.experimental import pallas as pl
from jax.experimental.pallas import tpu as pltpu
from jax.sharding import Mesh
from jax.sharding import PartitionSpec as P

eps = 1e-06
f32 = jnp.float32
bf16 = jnp.bfloat16

AXES = ("z", "yq", "ys", "x", "c")
Y = ("yq", "ys")
NZ, NY, NX, NC = 8, 8, 4, 2
ROWS = 32
HALF = 176
MAIN = 128
TAIL = 48
LANES = 640


def call(body, out_shape, *args, **kw):
    return pl.pallas_call(
        body,
        out_shape=out_shape,
        compiler_params=pltpu.CompilerParams(vmem_limit_bytes=56 * 1024 * 1024),
        **kw,
    )(*args)


def exchange(x, axis, size, phase):
    pairs = []
    for i in range(size):
        for c in range(NC):
            j = (i + 1) % size if (i + c + phase) % 2 == 0 else (i - 1) % size
            pairs.append((i * NC + c, j * NC + c))
    return lax.ppermute(x, (axis, "c"), pairs)


def dot_tt(left, right):
    return lax.dot_general(left, right, (((1,), (1,)), ((), ())), preferred_element_type=f32)


def dot_nn(left, right):
    return lax.dot_general(left, right, (((1,), (0,)), ((), ())), preferred_element_type=f32)


def normalize(x, gain):
    xf = x.astype(f32)
    inv = lax.rsqrt(jnp.mean(xf * xf, axis=-1, keepdims=True) + eps)
    return inv, (xf * inv * gain).astype(bf16)


def turn_block(r_ref, o_ref):
    t = r_ref[...].reshape(NY * ROWS, LANES).T
    for i, at in enumerate((384, 432, 512)):
        o_ref[HALF * i : HALF * i + MAIN] = t[MAIN * i : MAIN * (i + 1)]
        o_ref[HALF * i + MAIN : HALF * (i + 1)] = t[at : at + TAIL]


def turn_back(f_ref, o_ref):
    f = f_ref[...]
    zero = jnp.zeros((32, 256), f.dtype)
    t = jnp.concatenate(
        [f[HALF * i : HALF * i + MAIN] for i in range(3)]
        + [f[HALF * i + MAIN : HALF * (i + 1)] for i in range(2)]
        + [zero, f[2 * HALF + MAIN : 3 * HALF], zero, zero, zero[:16]],
        axis=0,
    ).T
    o_ref[...] = t.reshape(NY, ROWS, LANES).astype(o_ref.dtype)


def forward_part(b_ref, ta, tb, tc, td, p0, p1, p2, te, th, tl, acc, w):
    for q, piece in enumerate((ta, tb, tc, td)):
        for n in range(2):
            rows = pl.ds((q * 2 + n) * 48, 48)
            for k in range(8):
                cols = pl.ds(pl.multiple_of(b_ref[k] * 256, 256), 256)
                out = pl.ds(k * 256, 256)
                te[rows, out] = piece[n, 0, :, cols]
                th[rows, out] = piece[n, 1, :, cols]
                tl[rows, out] = piece[n, 2, :, cols]
    for q, pair in enumerate((p0, p1, p2)):
        for n in range(2):
            w[:, pl.ds((2 * q + n) * 256, 256)] = pair[n]
    k = 6 * 256
    g, u, d = w[0:HALF], w[HALF : 2 * HALF], w[2 * HALF : 3 * HALF]
    acc[0] = dot_tt(te[:, :k], g)
    acc[1] = dot_tt(te[:, :k], u)
    acc[2] = dot_tt(th[:, :k], d)
    acc[3] = dot_tt(tl[:, :k], g)
    acc[4] = dot_tt(tl[:, :k], u)


def forward_rest(acc, te, th, tl, p3, dg_ref, du_ref, hl_ref, at_ref, s_ref, w):
    for n in range(2):
        w[:, pl.ds(n * 256, 256)] = p3[n]
    k = 6 * 256
    g, u, d = w[0:HALF], w[HALF : 2 * HALF], w[2 * HALF : 3 * HALF]
    gate = acc[0] + dot_tt(te[:, k:], g)
    up = acc[1] + dot_tt(te[:, k:], u)
    dh = acc[2] + dot_tt(th[:, k:], d)
    sig = jax.nn.sigmoid(gate)
    silu = gate * sig
    hidden = (silu * up).astype(bf16)
    dg = (dh * up * sig * (1.0 + gate * (1.0 - sig))).astype(bf16)
    du = (dh * silu).astype(bf16)
    dg_ref[...] = dg
    du_ref[...] = du
    at_ref[0:HALF] = dg.T
    at_ref[HALF : 2 * HALF] = du.T
    at_ref[2 * HALF : 3 * HALF] = hidden.T
    for n in range(2):
        cols = pl.ds(k + n * 256, 256)
        s_ref[n, 0 : 2 * HALF] = dot_nn(at_ref[0 : 2 * HALF], te[:, cols]).astype(bf16)
        s_ref[n, 2 * HALF : 3 * HALF] = dot_nn(at_ref[2 * HALF : 3 * HALF], th[:, cols]).astype(bf16)
    gl = acc[3] + dot_tt(tl[:, k:], g)
    ul = acc[4] + dot_tt(tl[:, k:], u)
    hl_ref[...] = (gl * jax.nn.sigmoid(gl) * ul).astype(bf16)


def weight_grads(at_ref, te, th, o_ref):
    for n in range(6):
        cols = pl.ds(n * 256, 256)
        o_ref[n, 0 : 2 * HALF] = dot_nn(at_ref[0 : 2 * HALF], te[:, cols])
        o_ref[n, 2 * HALF : 3 * HALF] = dot_nn(at_ref[2 * HALF : 3 * HALF], th[:, cols])


def token_parts(b_ref, dg_ref, du_ref, hl_ref, p0, p1, p2, p3, o_ref):
    dg, du, hl = dg_ref[...], du_ref[...], hl_ref[...]
    for q, pair in enumerate((p0, p1, p2, p3)):
        for n in range(2):
            cols = pl.ds(pl.multiple_of(b_ref[2 * q + n] * 256, 256), 256)
            o_ref[0, :, cols] = dot_nn(hl, pair[n, 2 * HALF : 3 * HALF]).astype(bf16)
            o_ref[1, :, cols] = (
                dot_nn(dg, pair[n, 0:HALF]) + dot_nn(du, pair[n, HALF : 2 * HALF])
            ).astype(bf16)


def shape(dims, dtype=bf16):
    return jax.ShapeDtypeStruct(dims, dtype)


VM = pl.BlockSpec(memory_space=pltpu.VMEM)
SM = pl.BlockSpec(memory_space=pltpu.SMEM)


def packed(gate, up, down, h):
    cut = [a[:, h * MAIN : (h + 1) * MAIN] for a in (gate, up, down)]
    tail = [a[:, 256 + h * TAIL : 256 + (h + 1) * TAIL] for a in (gate, up, down)]
    zero = jnp.zeros((ROWS, 80), gate.dtype)
    return jnp.concatenate(cut + tail[:2] + [zero[:, :32], tail[2], zero], axis=1)


def on_device(
    x_late,
    x_early,
    cotangent,
    norm_gain,
    gate_weight,
    up_weight,
    down_weight,
    gate_sum,
    up_sum,
    down_sum,
):
    gain = norm_gain.astype(f32)
    z, c = lax.axis_index("z"), lax.axis_index("c")
    step = 1 - 2 * lax.rem(z + c, 2)
    order = jnp.array([0, 1, -1, -2, 2, 3, -3, -4], jnp.int32)
    blocks = lax.rem(z + order * step + 8, 8).astype(jnp.int32)

    halves = jnp.stack([packed(gate_weight, up_weight, down_weight, h) for h in range(2)])
    sent = jnp.tile(halves, (4, 1, 1))
    got = lax.all_to_all(sent, Y, split_axis=0, concat_axis=0, tiled=True)
    own = call(turn_block, shape((3 * HALF, 256)), got)
    p0 = jnp.stack([own, exchange(own, "z", NZ, 0)])
    p1 = exchange(p0, "z", NZ, 1)
    p2 = exchange(p1, "z", NZ, 0)
    p3 = exchange(p2, "z", NZ, 1)

    _, normed_late = normalize(x_late, gain)
    early_inv, normed_early = normalize(x_early, gain)
    half_cot = (0.5 * cotangent.astype(f32)).astype(bf16)
    tok = jnp.stack([normed_early, half_cot, normed_late])
    mate = lax.ppermute(tok, "ys", [(0, 1), (1, 0)])
    t0 = jnp.concatenate([tok, mate], axis=1)
    ta = jnp.stack([t0, exchange(t0, "x", NX, 0)])
    tb = exchange(ta, "x", NX, 1)
    swap = [(0, 1), (1, 0)]
    tc = lax.ppermute(ta, "c", swap)
    td = lax.ppermute(tb, "c", swap)

    te, th, tl, acc = call(
        forward_part,
        (shape((384, 2048)), shape((384, 2048)), shape((384, 2048)), shape((5, 384, HALF), f32)),
        blocks, ta, tb, tc, td, p0, p1, p2,
        in_specs=[SM] + [VM] * 7,
        scratch_shapes=[pltpu.VMEM((3 * HALF, 6 * 256), bf16)],
    )
    dg, du, hl, at, s3 = call(
        forward_rest,
        (shape((384, HALF)), shape((384, HALF)), shape((384, HALF)), shape((3 * HALF, 384)), shape((2, 3 * HALF, 256))),
        acc, te, th, tl, p3,
        scratch_shapes=[pltpu.VMEM((3 * HALF, 512), bf16)],
    )
    r3 = exchange(s3, "z", NZ, 1)
    parts = call(weight_grads, shape((6, 3 * HALF, 256), f32), at, te, th)
    outs = call(
        token_parts,
        shape((2, 384, 2048)),
        blocks, dg, du, hl, p0, p1, p2, p3,
        in_specs=[SM] + [VM] * 7,
    )
    r2 = exchange((parts[4:6] + r3.astype(f32)).astype(bf16), "z", NZ, 0)
    r1 = exchange((parts[2:4] + r2.astype(f32)).astype(bf16), "z", NZ, 1)
    a0 = parts[0:2] + r1.astype(f32)
    r0 = exchange(a0[1].astype(bf16), "z", NZ, 0)
    block = a0[0] + r0.astype(f32)
    back = call(turn_back, shape((NY, ROWS, LANES)), block)
    pieces = lax.all_to_all(back, Y, split_axis=0, concat_axis=0, tiled=True)
    total = jnp.sum(pieces.reshape(4, 2, ROWS, LANES).astype(f32), axis=0)

    def unpacked(i, running):
        at = (384, 432, 512)[i]
        return running + jnp.concatenate(
            [total[h, :, MAIN * i : MAIN * (i + 1)] for h in range(2)]
            + [total[h, :, at : at + TAIL] for h in range(2)],
            axis=1,
        )

    far = lax.ppermute(outs[:, 192:], "c", swap)
    near = outs[:, :192].astype(f32) + far.astype(f32)
    fx1 = exchange(near[:, 96:].astype(bf16), "x", NX, 1)
    near = near[:, :96] + fx1.astype(f32)
    fx0 = exchange(near[:, 48:].astype(bf16), "x", NX, 0)
    near = near[:, :48] + fx0.astype(f32)
    fy = lax.ppermute(near[:, 24:].astype(bf16), "ys", [(0, 1), (1, 0)])
    near = near[:, :24] + fy.astype(f32)
    branch, d_normed = near[0], near[1]
    out_late = (x_late.astype(f32) + 0.5 * branch).astype(bf16)
    early_f = x_early.astype(f32)
    scaled = d_normed * gain
    d_input = early_inv * scaled - early_f * early_inv**3 * jnp.mean(
        scaled * early_f, axis=-1, keepdims=True
    )
    grad_early = (cotangent.astype(f32) + d_input).astype(bf16)
    return (
        out_late,
        grad_early,
        unpacked(0, gate_sum),
        unpacked(1, up_sum),
        unpacked(2, down_sum),
    )


def solution(mesh):
    fine = Mesh(mesh.devices.reshape(NZ, 4, 2, NX, NC), AXES)
    token = P(AXES, None)
    weight = P(("z", "yq", "ys"), ("x", "c"))
    return jax.shard_map(
        on_device,
        mesh=fine,
        in_specs=(token, token, token, P()) + (weight,) * 6,
        out_specs=(token, token) + (weight,) * 3,
        check_vma=False,
    )
```

```python
import functools

import jax
import jax.numpy as jnp
from jax import lax
from jax.experimental import pallas as pl
from jax.experimental.pallas import tpu as pltpu
from jax.sharding import Mesh
from jax.sharding import PartitionSpec as P

eps = 1e-06
f32 = jnp.float32
bf16 = jnp.bfloat16

AXES = ("z", "yq", "ys", "x", "c")
Y = ("yq", "ys")
NZ, NY, NX, NC = 8, 8, 4, 2
ROWS = 32
HALF = 176
MAIN = 128
TAIL = 48
LANES = 640


def call(body, out_shape, *args, mib=16, **kw):
    return pl.pallas_call(
        body,
        out_shape=out_shape,
        compiler_params=pltpu.CompilerParams(vmem_limit_bytes=mib * 1024 * 1024),
        **kw,
    )(*args)


def exchange(x, axis, size, phase):
    pairs = []
    for i in range(size):
        for c in range(NC):
            j = (i + 1) % size if (i + c + phase) % 2 == 0 else (i - 1) % size
            pairs.append((i * NC + c, j * NC + c))
    return lax.ppermute(x, (axis, "c"), pairs)


def dot_tt(left, right):
    return lax.dot_general(left, right, (((1,), (1,)), ((), ())), preferred_element_type=f32)


def dot_nn(left, right):
    return lax.dot_general(left, right, (((1,), (0,)), ((), ())), preferred_element_type=f32)


def lanes_below(n):
    return lax.broadcasted_iota(jnp.int32, (ROWS, 128), 1) < n


def pack_weights(g_ref, u_ref, d_ref, o_ref):
    last = []
    for r in (g_ref, u_ref, d_ref):
        r = r[...].astype(f32)
        last.append(jnp.concatenate([r[:, 256:352], jnp.zeros((ROWS, 32), f32)], axis=1))
    g, u, d = last
    for h in range(2):
        if h == 0:
            t3 = jnp.where(lanes_below(48), g, pltpu.roll(u, 48, 1))
            t4 = d
        else:
            t3 = jnp.where(lanes_below(48), pltpu.roll(g, 80, 1), u)
            t4 = pltpu.roll(d, 80, 1)
        t3 = jnp.where(lanes_below(96), t3, 0.0).astype(bf16)
        t4 = jnp.where(lanes_below(48), t4, 0.0).astype(bf16)
        for q in range(4):
            for i, r in enumerate((g_ref, u_ref, d_ref)):
                o_ref[2 * q + h, :, MAIN * i : MAIN * (i + 1)] = r[:, h * MAIN : (h + 1) * MAIN]
            o_ref[2 * q + h, :, 384:512] = t3
            o_ref[2 * q + h, :, 512:640] = t4


def normalize(x, gain):
    inv = lax.rsqrt(jnp.mean(x * x, axis=-1, keepdims=True) + eps)
    return inv, x * inv * gain


def prepare_tokens(e_ref, c_ref, l_ref, g_ref, o_ref):
    gain = g_ref[...].astype(f32)
    o_ref[0] = normalize(e_ref[...].astype(f32), gain)[1].astype(bf16)
    o_ref[1] = (0.5 * c_ref[...].astype(f32)).astype(bf16)
    o_ref[2] = normalize(l_ref[...].astype(f32), gain)[1].astype(bf16)


def turn_block(r_ref, o_ref):
    t = r_ref[...].reshape(NY * ROWS, LANES).T
    for i, at in enumerate((384, 432, 512)):
        o_ref[HALF * i : HALF * i + MAIN] = t[MAIN * i : MAIN * (i + 1)]
        o_ref[HALF * i + MAIN : HALF * (i + 1)] = t[at : at + TAIL]


def join(a_ref, b_ref, o_ref):
    o_ref[0] = a_ref[...]
    o_ref[1] = b_ref[...]


def turned(f):
    zero = jnp.zeros((32, 256), f.dtype)
    return jnp.concatenate(
        [f[HALF * i : HALF * i + MAIN] for i in range(3)]
        + [f[HALF * i + MAIN : HALF * (i + 1)] for i in range(2)]
        + [zero, f[2 * HALF + MAIN : 3 * HALF], zero, zero, zero[:16]],
        axis=0,
    ).T


def forward_part(b_ref, ta, tb, tc, td, p0, p1, p2, te, th, tl, acc, w):
    for q, piece in enumerate((ta, tb, tc, td)):
        for n in range(2):
            rows = pl.ds((q * 2 + n) * 48, 48)
            for k in range(8):
                cols = pl.ds(pl.multiple_of(b_ref[k] * 256, 256), 256)
                out = pl.ds(k * 256, 256)
                te[rows, out] = piece[n, 0, :, cols]
                th[rows, out] = piece[n, 1, :, cols]
                tl[rows, out] = piece[n, 2, :, cols]
    for q, pair in enumerate((p0, p1, p2)):
        for n in range(2):
            w[:, pl.ds((2 * q + n) * 256, 256)] = pair[n]
    k = 6 * 256
    g, u, d = w[0:HALF], w[HALF : 2 * HALF], w[2 * HALF : 3 * HALF]
    acc[0] = dot_tt(te[:, :k], g)
    acc[1] = dot_tt(te[:, :k], u)
    acc[2] = dot_tt(th[:, :k], d)
    acc[3] = dot_tt(tl[:, :k], g)
    acc[4] = dot_tt(tl[:, :k], u)


def grad_block(at_ref, te, th, k, o, n, add=None):
    cols = pl.ds(k * 256, 256)
    up = dot_nn(at_ref[0 : 2 * HALF], te[:, cols])
    down = dot_nn(at_ref[2 * HALF : 3 * HALF], th[:, cols])
    if add is not None:
        up = up + add[0 : 2 * HALF].astype(f32)
        down = down + add[2 * HALF : 3 * HALF].astype(f32)
    o[n, 0 : 2 * HALF] = up.astype(o.dtype)
    o[n, 2 * HALF : 3 * HALF] = down.astype(o.dtype)


def early_rest(acc, te, th, p3, dg_ref, du_ref, at_ref, s_ref, w):
    for n in range(2):
        w[:, pl.ds(n * 256, 256)] = p3[n]
    k = 6 * 256
    gate = acc[0] + dot_tt(te[:, k:], w[0:HALF])
    up = acc[1] + dot_tt(te[:, k:], w[HALF : 2 * HALF])
    dh = acc[2] + dot_tt(th[:, k:], w[2 * HALF : 3 * HALF])
    sig = jax.nn.sigmoid(gate)
    silu = gate * sig
    hidden = (silu * up).astype(bf16)
    dg = (dh * up * sig * (1.0 + gate * (1.0 - sig))).astype(bf16)
    du = (dh * silu).astype(bf16)
    dg_ref[...] = dg
    du_ref[...] = du
    at_ref[0:HALF] = dg.T
    at_ref[HALF : 2 * HALF] = du.T
    at_ref[2 * HALF : 3 * HALF] = hidden.T
    for n in range(2):
        grad_block(at_ref, te, th, 6 + n, s_ref, n)


def add_pair(k, at_ref, te, th, r_ref, o_ref):
    for n in range(2):
        grad_block(at_ref, te, th, k + n, o_ref, n, r_ref[n])


def add_second(at_ref, te, th, r_ref, o_ref):
    grad_block(at_ref, te, th, 1, o_ref, 0, r_ref[1])


def own_block(at_ref, te, th, r_ref, o_ref, f):
    grad_block(at_ref, te, th, 0, f, 0, r_ref[0])
    o_ref[...] = turned(f[0])


def last_block(f_ref, r_ref, o_ref):
    t = f_ref[...] + turned(r_ref[0].astype(f32))
    o_ref[...] = t.reshape(NY, ROWS, LANES).astype(bf16)


def token_parts(b_ref, dg_ref, du_ref, acc, tl, p0, p1, p2, p3, near, far):
    k = 6 * 256
    gl, ul = acc[3], acc[4]
    for n in range(2):
        cols = pl.ds(k + n * 256, 256)
        gl = gl + dot_tt(tl[:, cols], p3[n, 0:HALF])
        ul = ul + dot_tt(tl[:, cols], p3[n, HALF : 2 * HALF])
    hl = (gl * jax.nn.sigmoid(gl) * ul).astype(bf16)
    dg, du = dg_ref[...], du_ref[...]
    for q, pair in enumerate((p0, p1, p2, p3)):
        for n in range(2):
            cols = pl.ds(pl.multiple_of(b_ref[2 * q + n] * 256, 256), 256)
            late = dot_nn(hl, pair[n, 2 * HALF : 3 * HALF])
            early = dot_nn(dg, pair[n, 0:HALF]) + dot_nn(du, pair[n, HALF : 2 * HALF])
            near[0, :, cols] = late[:192]
            near[1, :, cols] = early[:192]
            far[0, :, cols] = late[192:].astype(bf16)
            far[1, :, cols] = early[192:].astype(bf16)


def fold(n_ref, r_ref, keep, send):
    rows = keep.shape[1]
    for i in range(2):
        keep[i] = n_ref[i, :rows] + r_ref[i, :rows].astype(f32)
        send[i] = (n_ref[i, rows:] + r_ref[i, rows:].astype(f32)).astype(bf16)


def finish_tokens(n_ref, r_ref, e_ref, c_ref, l_ref, g_ref, late, early):
    gain = g_ref[...].astype(f32)
    branch = n_ref[0] + r_ref[0].astype(f32)
    late[...] = (l_ref[...].astype(f32) + 0.5 * branch).astype(bf16)
    d_normed = n_ref[1] + r_ref[1].astype(f32)
    x = e_ref[...].astype(f32)
    inv, _ = normalize(x, gain)
    scaled = d_normed * gain
    d_input = inv * scaled - x * inv**3 * jnp.mean(scaled * x, axis=-1, keepdims=True)
    early[...] = (c_ref[...].astype(f32) + d_input).astype(bf16)


def finish_weights(r_ref, gs, us, ds, go, uo, do):
    total = []
    for h in range(2):
        t = r_ref[h].astype(f32)
        for q in range(1, 4):
            t = t + r_ref[2 * q + h].astype(f32)
        total.append(t)
    t3 = [t[:, 384:512] for t in total]
    t4 = [t[:, 512:640] for t in total]
    low = lanes_below(48)
    g2 = jnp.where(low, t3[0], pltpu.roll(t3[1], 48, 1))
    u2 = jnp.where(low, pltpu.roll(t3[0], 80, 1), t3[1])
    d2 = jnp.where(low, t4[0], pltpu.roll(t4[1], 48, 1))
    for i, (s, o, t2) in enumerate(((gs, go, g2), (us, uo, u2), (ds, do, d2))):
        for h in range(2):
            cols = slice(h * MAIN, (h + 1) * MAIN)
            o[:, cols] = s[:, cols] + total[h][:, i * MAIN : (i + 1) * MAIN]
        o[:, 256:352] = s[:, 256:352] + t2[:, :96]


def shape(dims, dtype=bf16):
    return jax.ShapeDtypeStruct(dims, dtype)


VM = pl.BlockSpec(memory_space=pltpu.VMEM)
SM = pl.BlockSpec(memory_space=pltpu.SMEM)


def on_device(
    x_late,
    x_early,
    cotangent,
    norm_gain,
    gate_weight,
    up_weight,
    down_weight,
    gate_sum,
    up_sum,
    down_sum,
):
    gain = norm_gain.reshape(1, -1)
    z, c = lax.axis_index("z"), lax.axis_index("c")
    step = 1 - 2 * lax.rem(z + c, 2)
    order = jnp.array([0, 1, -1, -2, 2, 3, -3, -4], jnp.int32)
    blocks = lax.rem(z + order * step + 8, 8).astype(jnp.int32)
    swap = [(0, 1), (1, 0)]

    sent = call(pack_weights, shape((NY, ROWS, LANES)), gate_weight, up_weight, down_weight)
    got = lax.all_to_all(sent, Y, split_axis=0, concat_axis=0, tiled=True)
    own = call(turn_block, shape((3 * HALF, 256)), got)
    p0 = call(join, shape((2, 3 * HALF, 256)), own, exchange(own, "z", NZ, 0))
    p1 = exchange(p0, "z", NZ, 1)
    p2 = exchange(p1, "z", NZ, 0)
    p3 = exchange(p2, "z", NZ, 1)

    tok = call(prepare_tokens, shape((3, 24, 2048)), x_early, cotangent, x_late, gain)
    mate = lax.ppermute(tok, "ys", swap)
    t0 = jnp.concatenate([tok, mate], axis=1)
    ta = jnp.stack([t0, exchange(t0, "x", NX, 0)])
    tb = exchange(ta, "x", NX, 1)
    tc = lax.ppermute(ta, "c", swap)
    td = lax.ppermute(tb, "c", swap)

    te, th, tl, acc = call(
        forward_part,
        (shape((384, 2048)), shape((384, 2048)), shape((384, 2048)), shape((5, 384, HALF), f32)),
        blocks, ta, tb, tc, td, p0, p1, p2,
        in_specs=[SM] + [VM] * 7,
        scratch_shapes=[pltpu.VMEM((3 * HALF, 6 * 256), bf16)],
        mib=24,
    )
    pair = shape((2, 3 * HALF, 256))
    dg, du, at, s3 = call(
        early_rest,
        (shape((384, HALF)), shape((384, HALF)), shape((3 * HALF, 384)), pair),
        acc, te, th, p3,
        scratch_shapes=[pltpu.VMEM((3 * HALF, 512), bf16)],
    )
    r3 = exchange(s3, "z", NZ, 1)
    near, far = call(
        token_parts,
        (shape((2, 192, 2048), f32), shape((2, 192, 2048))),
        blocks, dg, du, acc, tl, p0, p1, p2, p3,
        in_specs=[SM] + [VM] * 8,
        mib=20,
    )
    r2 = exchange(call(functools.partial(add_pair, 4), pair, at, te, th, r3), "z", NZ, 0)
    r1 = exchange(call(functools.partial(add_pair, 2), pair, at, te, th, r2), "z", NZ, 1)
    r0 = exchange(call(add_second, shape((1, 3 * HALF, 256)), at, te, th, r1), "z", NZ, 0)
    block = call(
        own_block,
        shape((256, LANES), f32),
        at, te, th, r1,
        scratch_shapes=[pltpu.VMEM((1, 3 * HALF, 256), f32)],
    )
    back = call(last_block, shape((NY, ROWS, LANES)), block, r0)
    pieces = lax.all_to_all(back, Y, split_axis=0, concat_axis=0, tiled=True)
    sums = call(
        finish_weights, (shape((ROWS, 352), f32),) * 3, pieces, gate_sum, up_sum, down_sum
    )

    def folded(near, far):
        dims = (2, near.shape[1] // 2, 2048)
        return call(fold, (shape(dims, f32), shape(dims)), near, far)

    near, far = folded(near, lax.ppermute(far, "c", swap))
    near, far = folded(near, exchange(far, "x", NX, 1))
    near, far = folded(near, exchange(far, "x", NX, 0))
    far = lax.ppermute(far, "ys", swap)
    late, early = call(
        finish_tokens, (shape((24, 2048)),) * 2, near, far, x_early, cotangent, x_late, gain
    )
    return (late, early, *sums)


def solution(mesh):
    fine = Mesh(mesh.devices.reshape(NZ, 4, 2, NX, NC), AXES)
    token = P(AXES, None)
    weight = P(("z", "yq", "ys"), ("x", "c"))
    return jax.shard_map(
        on_device,
        mesh=fine,
        in_specs=(token, token, token, P()) + (weight,) * 6,
        out_specs=(token, token) + (weight,) * 3,
        check_vma=False,
    )
```

```python
import functools

import jax
import jax.numpy as jnp
from jax import lax
from jax.experimental import pallas as pl
from jax.experimental.pallas import tpu as pltpu
from jax.sharding import Mesh
from jax.sharding import PartitionSpec as P


eps = 1e-06
f32 = jnp.float32
bf16 = jnp.bfloat16

AXES = ("z", "yq", "ys", "x", "c")
NZ, NY, NX, NC = 8, 8, 4, 2
ROWS = 32
HALF = 176
MAIN = 128
TAIL = 48
LANES = 640


def call(body, out_shape, *args, mib=16, **kw):
    return pl.pallas_call(
        body,
        out_shape=out_shape,
        compiler_params=pltpu.CompilerParams(vmem_limit_bytes=mib * 1024 * 1024),
        **kw,
    )(*args)


def exchange(x, axis, size, phase):
    pairs = []
    for i in range(size):
        for c in range(NC):
            j = (i + 1) % size if (i + c + phase) % 2 == 0 else (i - 1) % size
            pairs.append((i * NC + c, j * NC + c))
    return lax.ppermute(x, (axis, "c"), pairs)


def swapped(x, axis):
    return lax.ppermute(x, axis, [(0, 1), (1, 0)])


def over_y(x):
    return lax.all_to_all(x, ("yq", "ys"), split_axis=0, concat_axis=0, tiled=True)


def dot_tt(left, right):
    return lax.dot_general(left, right, (((1,), (1,)), ((), ())), preferred_element_type=f32)


def dot_nn(left, right):
    return lax.dot_general(left, right, (((1,), (0,)), ((), ())), preferred_element_type=f32)


def lanes_below(n):
    return lax.broadcasted_iota(jnp.int32, (ROWS, 128), 1) < n


def fetch(pairs, sem):
    copies = [pltpu.make_async_copy(a, b, sem.at[i]) for i, (a, b) in enumerate(pairs)]
    for copy in copies:
        copy.start()
    for copy in copies:
        copy.wait()


def pack_weights(g_hbm, u_hbm, d_hbm, o_ref, g_ref, u_ref, d_ref, sem):
    fetch(((g_hbm, g_ref), (u_hbm, u_ref), (d_hbm, d_ref)), sem)
    last = []
    for r in (g_ref, u_ref, d_ref):
        r = r[...].astype(f32)
        last.append(jnp.concatenate([r[:, 256:352], jnp.zeros((ROWS, 32), f32)], axis=1))
    g, u, d = last
    for h in range(2):
        if h == 0:
            t3 = jnp.where(lanes_below(48), g, pltpu.roll(u, 48, 1))
            t4 = d
        else:
            t3 = jnp.where(lanes_below(48), pltpu.roll(g, 80, 1), u)
            t4 = pltpu.roll(d, 80, 1)
        t3 = jnp.where(lanes_below(96), t3, 0.0).astype(bf16)
        t4 = jnp.where(lanes_below(48), t4, 0.0).astype(bf16)
        for q in range(4):
            for i, r in enumerate((g_ref, u_ref, d_ref)):
                o_ref[2 * q + h, :, MAIN * i : MAIN * (i + 1)] = r[:, h * MAIN : (h + 1) * MAIN]
            o_ref[2 * q + h, :, 384:512] = t3
            o_ref[2 * q + h, :, 512:640] = t4


def normalize(x, gain):
    inv = lax.rsqrt(jnp.mean(x * x, axis=-1, keepdims=True) + eps)
    return inv, x * inv * gain


def prepare_tokens(e_hbm, c_hbm, l_hbm, g_hbm, o_ref, e_ref, c_ref, l_ref, g_ref, sem):
    fetch(((e_hbm, e_ref), (c_hbm, c_ref), (l_hbm, l_ref), (g_hbm, g_ref)), sem)
    gain = g_ref[...].astype(f32)
    o_ref[0] = normalize(e_ref[...].astype(f32), gain)[1].astype(bf16)
    o_ref[1] = (0.5 * c_ref[...].astype(f32)).astype(bf16)
    o_ref[2] = normalize(l_ref[...].astype(f32), gain)[1].astype(bf16)


def turn_block(r_ref, o_ref):
    t = r_ref[...].reshape(NY * ROWS, LANES).T
    for i, at in enumerate((384, 432, 512)):
        o_ref[HALF * i : HALF * i + MAIN] = t[MAIN * i : MAIN * (i + 1)]
        o_ref[HALF * i + MAIN : HALF * (i + 1)] = t[at : at + TAIL]


def join(a_ref, b_ref, o_ref):
    o_ref[0] = a_ref[...]
    o_ref[1] = b_ref[...]


def turned(f):
    zero = jnp.zeros((32, 256), f.dtype)
    return jnp.concatenate(
        [f[HALF * i : HALF * i + MAIN] for i in range(3)]
        + [f[HALF * i + MAIN : HALF * (i + 1)] for i in range(2)]
        + [zero, f[2 * HALF + MAIN : 3 * HALF], zero, zero, zero[:16]],
        axis=0,
    ).T


def forward_part(b_ref, ta, tb, p0, p1, p2, te, th, tl, acc, w):
    for q, piece in enumerate((ta, tb)):
        for n in range(2):
            rows = pl.ds((q * 2 + n) * 48, 48)
            for k in range(8):
                cols = pl.ds(pl.multiple_of(b_ref[k] * 256, 256), 256)
                out = pl.ds(k * 256, 256)
                te[rows, out] = piece[n, 0, :, cols]
                th[rows, out] = piece[n, 1, :, cols]
                tl[rows, out] = piece[n, 2, :, cols]
    for q, pair in enumerate((p0, p1, p2)):
        for n in range(2):
            w[:, pl.ds((2 * q + n) * 256, 256)] = pair[n]
    k = 6 * 256
    g, u, d = w[0:HALF], w[HALF : 2 * HALF], w[2 * HALF : 3 * HALF]
    acc[0] = dot_tt(te[:, :k], g)
    acc[1] = dot_tt(te[:, :k], u)
    acc[2] = dot_tt(th[:, :k], d)


def grad_block(at_ref, te, th, k, o, n, add=None):
    cols = pl.ds(k * 256, 256)
    for rows, t in ((slice(0, 2 * HALF), te), (slice(2 * HALF, 3 * HALF), th)):
        sums = dot_nn(at_ref[0, rows], t[0][:, cols]) + dot_nn(at_ref[1, rows], t[1][:, cols])
        if add is not None:
            sums = sums + add[rows].astype(f32)
        o[n, rows] = sums.astype(o.dtype)


def early_rest(acc0, acc1, te0, te1, th0, th1, p3, dg_ref, du_ref, at_ref, s_ref, w):
    for n in range(2):
        w[:, pl.ds(n * 256, 256)] = p3[n]
    k = 6 * 256
    for h, (acc, te, th) in enumerate(((acc0, te0, th0), (acc1, te1, th1))):
        gate = acc[0] + dot_tt(te[:, k:], w[0:HALF])
        up = acc[1] + dot_tt(te[:, k:], w[HALF : 2 * HALF])
        dh = acc[2] + dot_tt(th[:, k:], w[2 * HALF : 3 * HALF])
        sig = jax.nn.sigmoid(gate)
        silu = gate * sig
        hidden = (silu * up).astype(bf16)
        dg = (dh * up * sig * (1.0 + gate * (1.0 - sig))).astype(bf16)
        du = (dh * silu).astype(bf16)
        dg_ref[h] = dg
        du_ref[h] = du
        at_ref[h, 0:HALF] = dg.T
        at_ref[h, HALF : 2 * HALF] = du.T
        at_ref[h, 2 * HALF : 3 * HALF] = hidden.T
    for n in range(2):
        grad_block(at_ref, (te0, te1), (th0, th1), 6 + n, s_ref, n)


def add_pair(k, at_ref, te0, te1, th0, th1, r_ref, o_ref):
    for n in range(2):
        grad_block(at_ref, (te0, te1), (th0, th1), k + n, o_ref, n, r_ref[n])


def add_second(at_ref, te0, te1, th0, th1, r_ref, o_ref):
    grad_block(at_ref, (te0, te1), (th0, th1), 1, o_ref, 0, r_ref[1])


def own_block(at_ref, te0, te1, th0, th1, r_ref, o_ref, f):
    grad_block(at_ref, (te0, te1), (th0, th1), 0, f, 0, r_ref[0])
    o_ref[...] = turned(f[0])


def last_block(f_ref, r_ref, o_ref):
    t = f_ref[...] + turned(r_ref[0]).astype(f32)
    o_ref[...] = t.reshape(NY, ROWS, LANES).astype(bf16)


def token_parts(b_ref, dg_ref, du_ref, tl0, tl1, p0, p1, p2, p3, near, far, w):
    pairs = (p0, p1, p2, p3)
    for q, pair in enumerate(pairs):
        for n in range(2):
            w[:, pl.ds((2 * q + n) * 256, 256)] = pair[n, 0 : 2 * HALF]
    for h, (tl, o) in enumerate(((tl0, near), (tl1, far))):
        gl = dot_tt(tl[...], w[0:HALF])
        ul = dot_tt(tl[...], w[HALF : 2 * HALF])
        hl = (gl * jax.nn.sigmoid(gl) * ul).astype(bf16)
        dg, du = dg_ref[h], du_ref[h]
        for q, pair in enumerate(pairs):
            for n in range(2):
                cols = pl.ds(pl.multiple_of(b_ref[2 * q + n] * 256, 256), 256)
                late = dot_nn(hl, pair[n, 2 * HALF : 3 * HALF])
                early = dot_nn(dg, pair[n, 0:HALF]) + dot_nn(du, pair[n, HALF : 2 * HALF])
                o[0, :, cols] = late.astype(o.dtype)
                o[1, :, cols] = early.astype(o.dtype)


def fold(n_ref, r_ref, keep, send):
    rows = keep.shape[1]
    for i in range(2):
        keep[i] = n_ref[i, :rows] + r_ref[i, :rows].astype(f32)
        send[i] = (n_ref[i, rows:] + r_ref[i, rows:].astype(f32)).astype(bf16)


def finish_tokens(n_ref, r_ref, e_ref, c_ref, l_ref, g_ref, late, early):
    gain = g_ref[...].astype(f32)
    branch = n_ref[0] + r_ref[0].astype(f32)
    late[...] = (l_ref[...].astype(f32) + 0.5 * branch).astype(bf16)
    d_normed = n_ref[1] + r_ref[1].astype(f32)
    x = e_ref[...].astype(f32)
    inv, _ = normalize(x, gain)
    scaled = d_normed * gain
    d_input = inv * scaled - x * inv**3 * jnp.mean(scaled * x, axis=-1, keepdims=True)
    early[...] = (c_ref[...].astype(f32) + d_input).astype(bf16)


def finish_weights(r_ref, gs, us, ds, go, uo, do):
    total = []
    for h in range(2):
        t = r_ref[h].astype(f32)
        for q in range(1, 4):
            t = t + r_ref[2 * q + h].astype(f32)
        total.append(t)
    t3 = [t[:, 384:512] for t in total]
    t4 = [t[:, 512:640] for t in total]
    low = lanes_below(48)
    g2 = jnp.where(low, t3[0], pltpu.roll(t3[1], 48, 1))
    u2 = jnp.where(low, pltpu.roll(t3[0], 80, 1), t3[1])
    d2 = jnp.where(low, t4[0], pltpu.roll(t4[1], 48, 1))
    for i, (s, o, t2) in enumerate(((gs, go, g2), (us, uo, u2), (ds, do, d2))):
        for h in range(2):
            cols = slice(h * MAIN, (h + 1) * MAIN)
            o[:, cols] = s[:, cols] + total[h][:, i * MAIN : (i + 1) * MAIN]
        o[:, 256:352] = s[:, 256:352] + t2[:, :96]


def shape(dims, dtype=bf16):
    return jax.ShapeDtypeStruct(dims, dtype)


VM = pl.BlockSpec(memory_space=pltpu.VMEM)
HB = pl.BlockSpec(memory_space=pltpu.MemorySpace.HBM)
SM = pl.BlockSpec(memory_space=pltpu.SMEM)


def on_device(
    x_late,
    x_early,
    cotangent,
    norm_gain,
    gate_weight,
    up_weight,
    down_weight,
    gate_sum,
    up_sum,
    down_sum,
):
    gain = norm_gain.reshape(1, -1)
    z, c = lax.axis_index("z"), lax.axis_index("c")
    step = 1 - 2 * lax.rem(z + c, 2)
    order = jnp.array([0, 1, -1, -2, 2, 3, -3, -4], jnp.int32)
    blocks = lax.rem(z + order * step + 8, 8).astype(jnp.int32)

    sent = call(
        pack_weights,
        shape((NY, ROWS, LANES)),
        *(pltpu.with_memory_space_constraint(w, pltpu.HBM) for w in (gate_weight, up_weight, down_weight)),
        in_specs=[HB] * 3,
        scratch_shapes=[pltpu.VMEM((ROWS, 352), bf16)] * 3 + [pltpu.SemaphoreType.DMA((3,))],
    )
    own = call(turn_block, shape((3 * HALF, 256)), over_y(sent))
    p0 = call(join, shape((2, 3 * HALF, 256)), own, exchange(own, "z", NZ, 0))
    p1 = exchange(p0, "z", NZ, 1)
    p2 = exchange(p1, "z", NZ, 0)
    p3 = exchange(p2, "z", NZ, 1)

    tok = call(
        prepare_tokens,
        shape((3, 24, 2048)),
        *(pltpu.with_memory_space_constraint(x, pltpu.HBM) for x in (x_early, cotangent, x_late, gain)),
        in_specs=[HB] * 4,
        scratch_shapes=[pltpu.VMEM((24, 2048), bf16)] * 3
        + [pltpu.VMEM((1, 2048), bf16), pltpu.SemaphoreType.DMA((4,))],
    )
    t0 = jnp.concatenate([tok, swapped(tok, "ys")], axis=1)
    ta = jnp.stack([t0, exchange(t0, "x", NX, 0)])
    tb = exchange(ta, "x", NX, 1)
    tc = swapped(ta, "c")
    td = swapped(tb, "c")

    def most(first, second):
        return call(
            forward_part,
            (shape((192, 2048)),) * 3 + (shape((3, 192, HALF), f32),),
            blocks, first, second, p0, p1, p2,
            in_specs=[SM] + [VM] * 5,
            scratch_shapes=[pltpu.VMEM((3 * HALF, 6 * 256), bf16)],
        )

    te0, th0, tl0, acc0 = most(ta, tb)
    te1, th1, tl1, acc1 = most(tc, td)
    pair = shape((2, 3 * HALF, 256))
    dg, du, at, s3 = call(
        early_rest,
        (shape((2, 192, HALF)), shape((2, 192, HALF)), shape((2, 3 * HALF, 192)), pair),
        acc0, acc1, te0, te1, th0, th1, p3,
        scratch_shapes=[pltpu.VMEM((3 * HALF, 512), bf16)],
    )
    tokens = (at, te0, te1, th0, th1)
    r3 = exchange(s3, "z", NZ, 1)
    near, far = call(
        token_parts,
        (shape((2, 192, 2048), f32), shape((2, 192, 2048))),
        blocks, dg, du, tl0, tl1, p0, p1, p2, p3,
        in_specs=[SM] + [VM] * 8,
        scratch_shapes=[pltpu.VMEM((2 * HALF, 2048), bf16)],
    )
    s2 = call(functools.partial(add_pair, 4), pair, *tokens, r3)
    r2 = exchange(s2, "z", NZ, 0)
    s1 = call(functools.partial(add_pair, 2), pair, *tokens, r2)
    r1 = exchange(s1, "z", NZ, 1)
    s0 = call(add_second, shape((1, 3 * HALF, 256)), *tokens, r1)
    r0 = exchange(s0, "z", NZ, 0)
    block = call(
        own_block,
        shape((256, LANES), f32),
        *tokens, r1,
        scratch_shapes=[pltpu.VMEM((1, 3 * HALF, 256), f32)],
    )
    back = call(last_block, shape((NY, ROWS, LANES)), block, r0)
    sums = call(
        finish_weights,
        (shape((ROWS, 352), f32),) * 3,
        over_y(back), gate_sum, up_sum, down_sum,
    )

    def folded(near, far):
        dims = (2, near.shape[1] // 2, 2048)
        return call(fold, (shape(dims, f32), shape(dims)), near, far)

    near, far = folded(near, swapped(far, "c"))
    near, far = folded(near, exchange(far, "x", NX, 1))
    near, far = folded(near, exchange(far, "x", NX, 0))
    late, early = call(
        finish_tokens,
        (shape((24, 2048)),) * 2,
        near, swapped(far, "ys"), x_early, cotangent, x_late, gain,
    )
    return (late, early, *sums)


def solution(mesh):
    fine = Mesh(mesh.devices.reshape(NZ, 4, 2, NX, NC), AXES)
    token = P(AXES, None)
    weight = P(("z", "yq", "ys"), ("x", "c"))
    return jax.shard_map(
        on_device,
        mesh=fine,
        in_specs=(token, token, token, P()) + (weight,) * 6,
        out_specs=(token, token) + (weight,) * 3,
        check_vma=False,
    )
```

```python
import functools

import jax
import jax.numpy as jnp
from jax import lax
from jax.experimental import pallas as pl
from jax.experimental.pallas import tpu as pltpu
from jax.sharding import Mesh
from jax.sharding import PartitionSpec as P


eps = 1e-06
f32 = jnp.float32
bf16 = jnp.bfloat16

AXES = ("z", "yq", "ys", "x", "c")
NZ, NY, NX, NC = 8, 8, 4, 2
ROWS = 32
HALF = 176
MAIN = 128
TAIL = 48
PACK = 136


def call(body, out_shape, *args, mib=16, **kw):
    return pl.pallas_call(
        body,
        out_shape=out_shape,
        compiler_params=pltpu.CompilerParams(vmem_limit_bytes=mib * 1024 * 1024),
        **kw,
    )(*args)


def exchange(x, axis, size, phase):
    pairs = []
    for i in range(size):
        for c in range(NC):
            j = (i + 1) % size if (i + c + phase) % 2 == 0 else (i - 1) % size
            pairs.append((i * NC + c, j * NC + c))
    return lax.ppermute(x, (axis, "c"), pairs)


def hop_two(x):
    pairs = []
    for i in range(NZ):
        for c in range(NC):
            j = (i - 2) % NZ if (i + c) % 2 == 0 else (i + 2) % NZ
            pairs.append((i * NC + c, j * NC + c))
    return lax.ppermute(x, ("z", "c"), pairs)


def swapped(x, axis):
    return lax.ppermute(x, axis, [(0, 1), (1, 0)])


def over_y(x):
    return lax.all_to_all(x, ("yq", "ys"), split_axis=0, concat_axis=0, tiled=True)


def dot_tt(left, right):
    return lax.dot_general(left, right, (((1,), (1,)), ((), ())), preferred_element_type=f32)


def dot_nn(left, right):
    return lax.dot_general(left, right, (((1,), (0,)), ((), ())), preferred_element_type=f32)


def pick(*parts):
    out = parts[-1][1]
    lane = lax.broadcasted_iota(jnp.int32, out.shape, out.ndim - 1)
    for bound, part in reversed(parts[:-1]):
        out = jnp.where(lane < bound, part, out)
    return out


def shift(x, by):
    return pltpu.roll(x, by % 128, x.ndim - 1)


def fold_rows(x, start, axis):
    rows = [lax.slice_in_dim(x, 8 * j, 8 * j + 8, axis=axis) for j in range(4)]
    rows = [(16 * j + 16, shift(r, 16 * j - start)) for j, r in enumerate(rows)]
    return pick(*rows, (128, jnp.zeros_like(rows[0][1])))


def unfold_rows(x, axis):
    return jnp.concatenate([shift(x, -16 * j) for j in range(4)], axis=axis)


def fetch(pairs, sem):
    copies = [pltpu.make_async_copy(a, b, sem.at[i]) for i, (a, b) in enumerate(pairs)]
    for copy in copies:
        copy.start()
    for copy in copies:
        copy.wait()


def normalize(x, gain):
    inv = lax.rsqrt(jnp.mean(x * x, axis=-1, keepdims=True) + eps)
    return inv, x * inv * gain


def pack_weights(g_hbm, u_hbm, d_hbm, o_ref, g_ref, u_ref, d_ref, sem):
    fetch(((g_hbm, g_ref), (u_hbm, u_ref), (d_hbm, d_ref)), sem)
    weights = (g_ref, u_ref, d_ref)
    tails = []
    for r in weights:
        tail = r[:, 256:352].astype(f32)
        tails.append(jnp.concatenate([tail, jnp.zeros((ROWS, 32), f32)], axis=1))
    g, u, d = tails
    for h in range(2):
        at = h * TAIL
        tail = pick((48, shift(g, -at)), (96, shift(u, 48 - at)), (128, shift(d, 96 - at)))
        rest = fold_rows(d, at + 32, 0)
        for q in range(4):
            for i, r in enumerate(weights):
                o_ref[2 * q + h, ROWS * i : ROWS * (i + 1)] = r[:, h * MAIN : (h + 1) * MAIN]
            o_ref[2 * q + h, 96:128] = tail.astype(bf16)
            o_ref[2 * q + h, 128:136] = rest.astype(bf16)


def prepare_tokens(e_hbm, c_hbm, l_hbm, g_hbm, o_ref, early, cot, late, gain, sem):
    fetch(((e_hbm, early), (c_hbm, cot), (l_hbm, late), (g_hbm, gain)), sem)
    gain = gain[...].astype(f32).reshape(1, 2048)
    o_ref[0] = normalize(early[...].astype(f32), gain)[1].astype(bf16)
    o_ref[1] = (0.5 * cot[...].astype(f32)).astype(bf16)
    o_ref[2] = normalize(late[...].astype(f32), gain)[1].astype(bf16)


def turn_block(r_ref, o_ref):
    tiles = [r_ref[:, 32 * i : 32 * (i + 1)].reshape(NY * ROWS, 128).T for i in range(4)]
    rest = unfold_rows(r_ref[:, 128:136].astype(f32), 1).reshape(NY * ROWS, 128).T
    for i in range(3):
        o_ref[HALF * i : HALF * i + MAIN] = tiles[i]
    tail = tiles[3]
    o_ref[128:176] = tail[0:48]
    o_ref[304:352] = tail[48:96]
    o_ref[480:512] = tail[96:128]
    o_ref[512:528] = rest[0:16].astype(bf16)


def join(a_ref, b_ref, o_ref):
    o_ref[0] = a_ref[...]
    o_ref[1] = b_ref[...]


def turned(f):
    parts = [f[HALF * i : HALF * i + MAIN] for i in range(3)]
    parts.append(jnp.concatenate([f[128:176], f[304:352], f[480:512]], axis=0))
    parts.append(jnp.concatenate([f[512:528], jnp.zeros((112, 256), f.dtype)], axis=0))
    parts = [p.T.reshape(NY, ROWS, 128).astype(f32) for p in parts]
    return jnp.concatenate([*parts[:4], fold_rows(parts[4], 0, 1)], axis=1)


def forward_part(b_ref, ta, tb, p0, p1, p2, te, th, tl, acc, w):
    for q, piece in enumerate((ta, tb)):
        for n in range(2):
            rows = pl.ds((q * 2 + n) * 48, 48)
            for k in range(8):
                cols = pl.ds(pl.multiple_of(b_ref[k] * 256, 256), 256)
                out = pl.ds(k * 256, 256)
                te[rows, out] = piece[n, 0, :, cols]
                th[rows, out] = piece[n, 1, :, cols]
                tl[rows, out] = piece[n, 2, :, cols]
    for q, pair in enumerate((p0, p1, p2)):
        for n in range(2):
            w[:, pl.ds((2 * q + n) * 256, 256)] = pair[n]
    k = 6 * 256
    g, u, d = w[0:HALF], w[HALF : 2 * HALF], w[2 * HALF : 3 * HALF]
    acc[0] = dot_tt(te[:, :k], g)
    acc[1] = dot_tt(te[:, :k], u)
    acc[2] = dot_tt(th[:, :k], d)


def grad_block(at_ref, te, th, k, o, n, add=None):
    cols = pl.ds(k * 256, 256)
    for rows, t in ((slice(0, 2 * HALF), te), (slice(2 * HALF, 3 * HALF), th)):
        sums = dot_nn(at_ref[0, rows], t[0][:, cols]) + dot_nn(at_ref[1, rows], t[1][:, cols])
        if add is not None:
            sums = sums + add[rows].astype(f32)
        o[n, rows] = sums.astype(o.dtype)


def early_rest(acc0, acc1, te0, te1, th0, th1, p3, dg_ref, du_ref, at_ref, s_ref, w):
    for n in range(2):
        w[:, pl.ds(n * 256, 256)] = p3[n]
    k = 6 * 256
    for h, (acc, te, th) in enumerate(((acc0, te0, th0), (acc1, te1, th1))):
        gate = acc[0] + dot_tt(te[:, k:], w[0:HALF])
        up = acc[1] + dot_tt(te[:, k:], w[HALF : 2 * HALF])
        dh = acc[2] + dot_tt(th[:, k:], w[2 * HALF : 3 * HALF])
        sig = jax.nn.sigmoid(gate)
        silu = gate * sig
        hidden = (silu * up).astype(bf16)
        dg = (dh * up * sig * (1.0 + gate * (1.0 - sig))).astype(bf16)
        du = (dh * silu).astype(bf16)
        dg_ref[h] = dg
        du_ref[h] = du
        at_ref[h, 0:HALF] = dg.T
        at_ref[h, HALF : 2 * HALF] = du.T
        at_ref[h, 2 * HALF : 3 * HALF] = hidden.T
    for n in range(2):
        grad_block(at_ref, (te0, te1), (th0, th1), 6 + n, s_ref, n)


def add_pair(k, at_ref, te0, te1, th0, th1, r_ref, o_ref):
    for n in range(2):
        grad_block(at_ref, (te0, te1), (th0, th1), k + n, o_ref, n, r_ref[n])


def add_each(at_ref, te0, te1, th0, th1, r_ref, o_ref, p_ref):
    for n, o in enumerate((o_ref, p_ref)):
        grad_block(at_ref, (te0, te1), (th0, th1), 2 + n, o, 0, r_ref[n])


def neighbour_share(at_ref, te0, te1, th0, th1, o_ref):
    grad_block(at_ref, (te0, te1), (th0, th1), 1, o_ref, 0)


def own_block(at_ref, te0, te1, th0, th1, r_ref, q_ref, o_ref, f):
    both = r_ref[0].astype(f32) + q_ref[0].astype(f32)
    grad_block(at_ref, (te0, te1), (th0, th1), 0, f, 0, both)
    o_ref[...] = turned(f[0])


def last_block(f_ref, r_ref, o_ref):
    o_ref[...] = (f_ref[...] + turned(r_ref[0])).astype(bf16)


def token_parts(b_ref, dg_ref, du_ref, tl0, tl1, p0, p1, p2, p3, near, far, w):
    pairs = (p0, p1, p2, p3)
    for q, pair in enumerate(pairs):
        for n in range(2):
            w[:, pl.ds((2 * q + n) * 256, 256)] = pair[n, 0 : 2 * HALF]
    for h, (tl, o) in enumerate(((tl0, near), (tl1, far))):
        gl = dot_tt(tl[...], w[0:HALF])
        ul = dot_tt(tl[...], w[HALF : 2 * HALF])
        hl = (gl * jax.nn.sigmoid(gl) * ul).astype(bf16)
        dg, du = dg_ref[h], du_ref[h]
        for q, pair in enumerate(pairs):
            for n in range(2):
                cols = pl.ds(pl.multiple_of(b_ref[2 * q + n] * 256, 256), 256)
                late = dot_nn(hl, pair[n, 2 * HALF : 3 * HALF])
                early = dot_nn(dg, pair[n, 0:HALF]) + dot_nn(du, pair[n, HALF : 2 * HALF])
                o[0, :, cols] = late.astype(o.dtype)
                o[1, :, cols] = early.astype(o.dtype)


def fold(n_ref, r_ref, keep, send):
    rows = keep.shape[1]
    for i in range(2):
        keep[i] = n_ref[i, :rows] + r_ref[i, :rows].astype(f32)
        send[i] = (n_ref[i, rows:] + r_ref[i, rows:].astype(f32)).astype(bf16)


def finish_tokens(n_ref, r_ref, e_ref, c_ref, l_ref, g_ref, late, early):
    gain = g_ref[...].astype(f32)
    branch = n_ref[0] + r_ref[0].astype(f32)
    late[...] = (l_ref[...].astype(f32) + 0.5 * branch).astype(bf16)
    d_normed = n_ref[1] + r_ref[1].astype(f32)
    x = e_ref[...].astype(f32)
    inv, _ = normalize(x, gain)
    scaled = d_normed * gain
    d_input = inv * scaled - x * inv**3 * jnp.mean(scaled * x, axis=-1, keepdims=True)
    early[...] = (c_ref[...].astype(f32) + d_input).astype(bf16)


def finish_weights(r_ref, gs, us, ds, go, uo, do):
    total = []
    for h in range(2):
        t = r_ref[h].astype(f32)
        for q in range(1, 4):
            t = t + r_ref[2 * q + h].astype(f32)
        total.append(t)
    t = [t[96:128] for t in total]
    r = [unfold_rows(t[128:136], 0) for t in total]
    g2 = pick((48, t[0]), (128, shift(t[1], 48)))
    u2 = pick((48, shift(t[0], -48)), (128, t[1]))
    d2 = pick((32, shift(t[0], 32)), (48, shift(r[0], 32)), (80, shift(t[1], 80)), (128, shift(r[1], 80)))
    for i, (s, o, t2) in enumerate(((gs, go, g2), (us, uo, u2), (ds, do, d2))):
        for h in range(2):
            cols = slice(h * MAIN, (h + 1) * MAIN)
            o[:, cols] = s[:, cols] + total[h][ROWS * i : ROWS * (i + 1)]
        o[:, 256:352] = s[:, 256:352] + t2[:, :96]


def shape(dims, dtype=bf16):
    return jax.ShapeDtypeStruct(dims, dtype)


VM = pl.BlockSpec(memory_space=pltpu.VMEM)
HB = pl.BlockSpec(memory_space=pltpu.MemorySpace.HBM)
SM = pl.BlockSpec(memory_space=pltpu.SMEM)


def on_device(
    x_late,
    x_early,
    cotangent,
    norm_gain,
    gate_weight,
    up_weight,
    down_weight,
    gate_sum,
    up_sum,
    down_sum,
):
    gain = norm_gain.reshape(1, -1)
    z, c = lax.axis_index("z"), lax.axis_index("c")
    step = 1 - 2 * lax.rem(z + c, 2)
    order = jnp.array([0, 1, -1, -2, 2, 3, -3, -4], jnp.int32)
    blocks = lax.rem(z + order * step + 8, 8).astype(jnp.int32)

    def staged(body, dims, *given):
        n = len(given)
        return call(
            body,
            shape(dims),
            *(pltpu.with_memory_space_constraint(a, pltpu.HBM) for a in given),
            in_specs=[HB] * n,
            scratch_shapes=[pltpu.VMEM(a.shape, bf16) for a in given]
            + [pltpu.SemaphoreType.DMA((n,))],
        )

    sent = staged(pack_weights, (NY, PACK, 128), gate_weight, up_weight, down_weight)
    tok = staged(prepare_tokens, (3, 24, 2048), x_early, cotangent, x_late, norm_gain)
    own = call(turn_block, shape((3 * HALF, 256)), over_y(sent))
    p0 = call(join, shape((2, 3 * HALF, 256)), own, exchange(own, "z", NZ, 0))
    p1 = exchange(p0, "z", NZ, 1)
    p2 = exchange(p1, "z", NZ, 0)
    p3 = exchange(p2, "z", NZ, 1)

    t0 = jnp.concatenate([tok, exchange(tok, "x", NX, 0)], axis=1)
    ta = jnp.stack([t0, swapped(t0, "ys")])
    tb = exchange(ta, "x", NX, 1)
    tc = swapped(ta, "c")
    td = swapped(tb, "c")

    def most(first, second):
        return call(
            forward_part,
            (shape((192, 2048)),) * 3 + (shape((3, 192, HALF), f32),),
            blocks, first, second, p0, p1, p2,
            in_specs=[SM] + [VM] * 5,
            scratch_shapes=[pltpu.VMEM((3 * HALF, 6 * 256), bf16)],
        )

    te0, th0, tl0, acc0 = most(ta, tb)
    te1, th1, tl1, acc1 = most(tc, td)
    pair = shape((2, 3 * HALF, 256))
    dg, du, at, s3 = call(
        early_rest,
        (shape((2, 192, HALF)), shape((2, 192, HALF)), shape((2, 3 * HALF, 192)), pair),
        acc0, acc1, te0, te1, th0, th1, p3,
        scratch_shapes=[pltpu.VMEM((3 * HALF, 512), bf16)],
    )
    tokens = (at, te0, te1, th0, th1)
    r3 = exchange(s3, "z", NZ, 1)
    near, far = call(
        token_parts,
        (shape((2, 192, 2048), f32), shape((2, 192, 2048))),
        blocks, dg, du, tl0, tl1, p0, p1, p2, p3,
        in_specs=[SM] + [VM] * 8,
        scratch_shapes=[pltpu.VMEM((2 * HALF, 2048), bf16)],
    )
    s2 = call(functools.partial(add_pair, 4), pair, *tokens, r3)
    r2 = exchange(s2, "z", NZ, 0)
    one = shape((1, 3 * HALF, 256))
    mine = exchange(call(neighbour_share, one, *tokens), "z", NZ, 0)
    s1, s0 = call(add_each, (one, one), *tokens, r2)
    r0 = hop_two(s0)
    r1 = exchange(s1, "z", NZ, 1)
    block = call(
        own_block,
        shape((NY, PACK, 128), f32),
        *tokens, mine, r1,
        scratch_shapes=[pltpu.VMEM((1, 3 * HALF, 256), f32)],
    )
    back = call(last_block, shape((NY, PACK, 128)), block, r0)
    sums = call(
        finish_weights,
        (shape((ROWS, 352), f32),) * 3,
        over_y(back), gate_sum, up_sum, down_sum,
    )

    def folded(near, far):
        dims = (2, near.shape[1] // 2, 2048)
        return call(fold, (shape(dims, f32), shape(dims)), near, far)

    near, far = folded(near, swapped(far, "c"))
    near, far = folded(near, exchange(far, "x", NX, 1))
    near, far = folded(near, swapped(far, "ys"))
    late, early = call(
        finish_tokens,
        (shape((24, 2048)),) * 2,
        near, exchange(far, "x", NX, 0), x_early, cotangent, x_late, gain,
    )
    return (late, early, *sums)


def solution(mesh):
    fine = Mesh(mesh.devices.reshape(NZ, 4, 2, NX, NC), AXES)
    token = P(AXES, None)
    weight = P(("z", "yq", "ys"), ("x", "c"))
    return jax.shard_map(
        on_device,
        mesh=fine,
        in_specs=(token, token, token, P()) + (weight,) * 6,
        out_specs=(token, token) + (weight,) * 3,
        check_vma=False,
    )
```

```python
import functools

import jax
import jax.numpy as jnp
from jax import lax
from jax.experimental import pallas as pl
from jax.experimental.pallas import tpu as pltpu
from jax.sharding import Mesh
from jax.sharding import PartitionSpec as P


eps = 1e-06
f32 = jnp.float32
bf16 = jnp.bfloat16

AXES = ("z", "yq", "ys", "x", "c")
NZ, NY, NX, NC = 8, 8, 4, 2
FLIP = {"z": 0, "x": 1}
ROWS = 32
HALF = 176
MAIN = 128
TAIL = 48
PACK = 136


def call(body, out_shape, *args, mib=16, **kw):
    return pl.pallas_call(
        body,
        out_shape=out_shape,
        compiler_params=pltpu.CompilerParams(vmem_limit_bytes=mib * 1024 * 1024),
        **kw,
    )(*args)


def exchange(x, axis, size, phase):
    pairs = []
    for i in range(size):
        for c in range(NC):
            j = (i + 1) % size if (i + c + phase + FLIP[axis]) % 2 == 0 else (i - 1) % size
            pairs.append((i * NC + c, j * NC + c))
    return lax.ppermute(x, (axis, "c"), pairs)


def hop_two(x, way):
    pairs = []
    for i in range(NZ):
        for c in range(NC):
            j = (i + 2 * way) % NZ if (i + c + FLIP["z"]) % 2 == 0 else (i - 2 * way) % NZ
            pairs.append((i * NC + c, j * NC + c))
    return lax.ppermute(x, ("z", "c"), pairs)


def swapped(x, axis):
    return lax.ppermute(x, axis, [(0, 1), (1, 0)])


def over_y(x):
    return lax.all_to_all(x, ("yq", "ys"), split_axis=0, concat_axis=0, tiled=True)


def dot_tt(left, right):
    return lax.dot_general(left, right, (((1,), (1,)), ((), ())), preferred_element_type=f32)


def dot_nn(left, right):
    return lax.dot_general(left, right, (((1,), (0,)), ((), ())), preferred_element_type=f32)


def pick(*parts):
    out = parts[-1][1]
    lane = lax.broadcasted_iota(jnp.int32, out.shape, out.ndim - 1)
    for bound, part in reversed(parts[:-1]):
        out = jnp.where(lane < bound, part, out)
    return out


def shift(x, by):
    return pltpu.roll(x, by % 128, x.ndim - 1)


def fold_rows(x, start, axis):
    rows = [lax.slice_in_dim(x, 8 * j, 8 * j + 8, axis=axis) for j in range(4)]
    rows = [(16 * j + 16, shift(r, 16 * j - start)) for j, r in enumerate(rows)]
    return pick(*rows, (128, jnp.zeros_like(rows[0][1])))


def unfold_rows(x, axis):
    return jnp.concatenate([shift(x, -16 * j) for j in range(4)], axis=axis)


def fetch(pairs, sem):
    copies = [pltpu.make_async_copy(a, b, sem.at[i]) for i, (a, b) in enumerate(pairs)]
    for copy in copies:
        copy.start()
    for copy in copies:
        copy.wait()


def normalize(x, gain):
    inv = lax.rsqrt(jnp.mean(x * x, axis=-1, keepdims=True) + eps)
    return inv, x * inv * gain


def pack_weights(g_hbm, u_hbm, d_hbm, o_ref, g_ref, u_ref, d_ref, sem):
    fetch(((g_hbm, g_ref), (u_hbm, u_ref), (d_hbm, d_ref)), sem)
    weights = (g_ref, u_ref, d_ref)
    tails = []
    for r in weights:
        tail = r[:, 256:352].astype(f32)
        tails.append(jnp.concatenate([tail, jnp.zeros((ROWS, 32), f32)], axis=1))
    g, u, d = tails
    for h in range(2):
        at = h * TAIL
        tail = pick((48, shift(g, -at)), (96, shift(u, 48 - at)), (128, shift(d, 96 - at)))
        rest = fold_rows(d, at + 32, 0)
        for q in range(4):
            for i, r in enumerate(weights):
                o_ref[2 * q + h, ROWS * i : ROWS * (i + 1)] = r[:, h * MAIN : (h + 1) * MAIN]
            o_ref[2 * q + h, 96:128] = tail.astype(bf16)
            o_ref[2 * q + h, 128:136] = rest.astype(bf16)


def prepare_tokens(e_hbm, c_hbm, l_hbm, g_hbm, o_ref, early, cot, late, gain, sem):
    fetch(((e_hbm, early), (c_hbm, cot), (l_hbm, late), (g_hbm, gain)), sem)
    gain = gain[...].astype(f32).reshape(1, 2048)
    o_ref[0] = normalize(early[...].astype(f32), gain)[1].astype(bf16)
    o_ref[1] = (0.5 * cot[...].astype(f32)).astype(bf16)
    o_ref[2] = normalize(late[...].astype(f32), gain)[1].astype(bf16)


def turn_block(r_ref, o_ref):
    tiles = [r_ref[:, 32 * i : 32 * (i + 1)].reshape(NY * ROWS, 128).T for i in range(4)]
    rest = unfold_rows(r_ref[:, 128:136].astype(f32), 1).reshape(NY * ROWS, 128).T
    for i in range(3):
        o_ref[HALF * i : HALF * i + MAIN] = tiles[i]
    tail = tiles[3]
    o_ref[128:176] = tail[0:48]
    o_ref[304:352] = tail[48:96]
    o_ref[480:512] = tail[96:128]
    o_ref[512:528] = rest[0:16].astype(bf16)


def join(a_ref, b_ref, o_ref):
    o_ref[0] = a_ref[...]
    o_ref[1] = b_ref[...]


def turned(f):
    parts = [f[HALF * i : HALF * i + MAIN] for i in range(3)]
    parts.append(jnp.concatenate([f[128:176], f[304:352], f[480:512]], axis=0))
    parts.append(jnp.concatenate([f[512:528], jnp.zeros((112, 256), f.dtype)], axis=0))
    parts = [p.T.reshape(NY, ROWS, 128).astype(f32) for p in parts]
    return jnp.concatenate([*parts[:4], fold_rows(parts[4], 0, 1)], axis=1)


def forward_part(b_ref, ta, tb, own, got, p1, p2, te, th, tl, acc, w):
    for q, piece in enumerate((ta, tb)):
        for n in range(2):
            rows = pl.ds((q * 2 + n) * 48, 48)
            for k in range(8):
                cols = pl.ds(pl.multiple_of(b_ref[k] * 256, 256), 256)
                out = pl.ds(k * 256, 256)
                te[rows, out] = piece[n, 0, :, cols]
                th[rows, out] = piece[n, 1, :, cols]
                tl[rows, out] = piece[n, 2, :, cols]
    for n, block in enumerate((own, got, p1.at[0], p1.at[1], p2.at[0], p2.at[1])):
        w[:, pl.ds(n * 256, 256)] = block[...]
    k = 6 * 256
    g, u, d = w[0:HALF], w[HALF : 2 * HALF], w[2 * HALF : 3 * HALF]
    acc[0] = dot_tt(te[:, :k], g)
    acc[1] = dot_tt(te[:, :k], u)
    acc[2] = dot_tt(th[:, :k], d)


def grad_block(at_ref, te, th, k, o, n, add=None):
    cols = pl.ds(k * 256, 256)
    for rows, t in ((slice(0, 2 * HALF), te), (slice(2 * HALF, 3 * HALF), th)):
        sums = dot_nn(at_ref[0, rows], t[0][:, cols]) + dot_nn(at_ref[1, rows], t[1][:, cols])
        if add is not None:
            sums = sums + add[rows].astype(f32)
        o[n, rows] = sums.astype(o.dtype)


def early_rest(acc0, acc1, te0, te1, th0, th1, p3, dg_ref, du_ref, at_ref, s_ref, w):
    for n in range(2):
        w[:, pl.ds(n * 256, 256)] = p3[n]
    k = 6 * 256
    for h, (acc, te, th) in enumerate(((acc0, te0, th0), (acc1, te1, th1))):
        gate = acc[0] + dot_tt(te[:, k:], w[0:HALF])
        up = acc[1] + dot_tt(te[:, k:], w[HALF : 2 * HALF])
        dh = acc[2] + dot_tt(th[:, k:], w[2 * HALF : 3 * HALF])
        sig = jax.nn.sigmoid(gate)
        silu = gate * sig
        hidden = (silu * up).astype(bf16)
        dg = (dh * up * sig * (1.0 + gate * (1.0 - sig))).astype(bf16)
        du = (dh * silu).astype(bf16)
        dg_ref[h] = dg
        du_ref[h] = du
        at_ref[h, 0:HALF] = dg.T
        at_ref[h, HALF : 2 * HALF] = du.T
        at_ref[h, 2 * HALF : 3 * HALF] = hidden.T
    for n in range(2):
        grad_block(at_ref, (te0, te1), (th0, th1), 6 + n, s_ref, n)


def add_pair(k, at_ref, te0, te1, th0, th1, r_ref, o_ref):
    for n in range(2):
        grad_block(at_ref, (te0, te1), (th0, th1), k + n, o_ref, n, r_ref[n])


def add_each(at_ref, te0, te1, th0, th1, r_ref, o_ref, p_ref):
    for n, o in enumerate((o_ref, p_ref)):
        grad_block(at_ref, (te0, te1), (th0, th1), 2 + n, o, 0, r_ref[n])


def neighbour_share(at_ref, te0, te1, th0, th1, o_ref):
    grad_block(at_ref, (te0, te1), (th0, th1), 1, o_ref, 0)


def own_block(at_ref, te0, te1, th0, th1, r_ref, q_ref, o_ref, f):
    both = r_ref[0].astype(f32) + q_ref[0].astype(f32)
    grad_block(at_ref, (te0, te1), (th0, th1), 0, f, 0, both)
    o_ref[...] = turned(f[0])


def last_block(f_ref, r_ref, o_ref):
    o_ref[...] = (f_ref[...] + turned(r_ref[0])).astype(bf16)


def token_parts(b_ref, dg_ref, du_ref, tl0, tl1, own, got, p1, p2, p3, near, far, w):
    blocks = (own, got) + tuple(p.at[n] for p in (p1, p2, p3) for n in range(2))
    for n, block in enumerate(blocks):
        w[:, pl.ds(n * 256, 256)] = block[0 : 2 * HALF]
    for h, (tl, o) in enumerate(((tl0, near), (tl1, far))):
        gl = dot_tt(tl[...], w[0:HALF])
        ul = dot_tt(tl[...], w[HALF : 2 * HALF])
        hl = (gl * jax.nn.sigmoid(gl) * ul).astype(bf16)
        dg, du = dg_ref[h], du_ref[h]
        for n, block in enumerate(blocks):
            cols = pl.ds(pl.multiple_of(b_ref[n] * 256, 256), 256)
            late = dot_nn(hl, block[2 * HALF : 3 * HALF])
            early = dot_nn(dg, block[0:HALF]) + dot_nn(du, block[HALF : 2 * HALF])
            o[0, :, cols] = late.astype(o.dtype)
            o[1, :, cols] = early.astype(o.dtype)


def fold(n_ref, r_ref, keep, send):
    rows = keep.shape[1]
    for i in range(2):
        keep[i] = n_ref[i, :rows] + r_ref[i, :rows].astype(f32)
        send[i] = (n_ref[i, rows:] + r_ref[i, rows:].astype(f32)).astype(bf16)


def fold_mate(n_ref, r_ref, keep, send):
    for i in range(2):
        sums = n_ref[i] + r_ref[i].astype(f32)
        keep[i] = jnp.concatenate([sums[0:24], sums[48:72]], axis=0)
        send[i] = jnp.concatenate([sums[24:48], sums[72:96]], axis=0).astype(bf16)


def finish_tokens(n_ref, r_ref, e_ref, c_ref, l_ref, g_ref, late, early):
    gain = g_ref[...].astype(f32)
    branch = n_ref[0] + r_ref[0].astype(f32)
    late[...] = (l_ref[...].astype(f32) + 0.5 * branch).astype(bf16)
    d_normed = n_ref[1] + r_ref[1].astype(f32)
    x = e_ref[...].astype(f32)
    inv, _ = normalize(x, gain)
    scaled = d_normed * gain
    d_input = inv * scaled - x * inv**3 * jnp.mean(scaled * x, axis=-1, keepdims=True)
    early[...] = (c_ref[...].astype(f32) + d_input).astype(bf16)


def finish_weights(r_ref, gs, us, ds, go, uo, do):
    total = []
    for h in range(2):
        t = r_ref[h].astype(f32)
        for q in range(1, 4):
            t = t + r_ref[2 * q + h].astype(f32)
        total.append(t)
    t = [t[96:128] for t in total]
    r = [unfold_rows(t[128:136], 0) for t in total]
    g2 = pick((48, t[0]), (128, shift(t[1], 48)))
    u2 = pick((48, shift(t[0], -48)), (128, t[1]))
    d2 = pick((32, shift(t[0], 32)), (48, shift(r[0], 32)), (80, shift(t[1], 80)), (128, shift(r[1], 80)))
    for i, (s, o, t2) in enumerate(((gs, go, g2), (us, uo, u2), (ds, do, d2))):
        for h in range(2):
            cols = slice(h * MAIN, (h + 1) * MAIN)
            o[:, cols] = s[:, cols] + total[h][ROWS * i : ROWS * (i + 1)]
        o[:, 256:352] = s[:, 256:352] + t2[:, :96]


def shape(dims, dtype=bf16):
    return jax.ShapeDtypeStruct(dims, dtype)


VM = pl.BlockSpec(memory_space=pltpu.VMEM)
HB = pl.BlockSpec(memory_space=pltpu.MemorySpace.HBM)
SM = pl.BlockSpec(memory_space=pltpu.SMEM)


def on_device(
    x_late,
    x_early,
    cotangent,
    norm_gain,
    gate_weight,
    up_weight,
    down_weight,
    gate_sum,
    up_sum,
    down_sum,
):
    gain = norm_gain.reshape(1, -1)
    z, c = lax.axis_index("z"), lax.axis_index("c")
    step = 1 - 2 * lax.rem(z + c + FLIP["z"], 2)
    order = jnp.array([0, 1, -1, -2, 2, 3, -3, -4], jnp.int32)
    blocks = lax.rem(z + order * step + 8, 8).astype(jnp.int32)

    def staged(body, dims, *given):
        n = len(given)
        return call(
            body,
            shape(dims),
            *(pltpu.with_memory_space_constraint(a, pltpu.HBM) for a in given),
            in_specs=[HB] * n,
            scratch_shapes=[pltpu.VMEM(a.shape, bf16) for a in given]
            + [pltpu.SemaphoreType.DMA((n,))],
        )

    sent = staged(pack_weights, (NY, PACK, 128), gate_weight, up_weight, down_weight)
    tok = staged(prepare_tokens, (3, 24, 2048), x_early, cotangent, x_late, norm_gain)
    own = call(turn_block, shape((3 * HALF, 256)), over_y(sent))
    got = exchange(own, "z", NZ, 0)
    far = hop_two(own, 1)
    p1 = call(join, shape((2, 3 * HALF, 256)), exchange(own, "z", NZ, 1), far)
    p2 = exchange(p1, "z", NZ, 0)
    p3 = exchange(p2, "z", NZ, 1)

    t0 = jnp.concatenate([tok, swapped(tok, "ys")], axis=1)
    ta = call(join, shape((2, 3, 48, 2048)), t0, exchange(t0, "x", NX, 0))
    tb = exchange(ta, "x", NX, 1)
    tc = swapped(ta, "c")
    td = swapped(tb, "c")

    def most(first, second):
        return call(
            forward_part,
            (shape((192, 2048)),) * 3 + (shape((3, 192, HALF), f32),),
            blocks, first, second, own, got, p1, p2,
            in_specs=[SM] + [VM] * 6,
            scratch_shapes=[pltpu.VMEM((3 * HALF, 6 * 256), bf16)],
        )

    te0, th0, tl0, acc0 = most(ta, tb)
    te1, th1, tl1, acc1 = most(tc, td)
    pair = shape((2, 3 * HALF, 256))
    dg, du, at, s3 = call(
        early_rest,
        (shape((2, 192, HALF)), shape((2, 192, HALF)), shape((2, 3 * HALF, 192)), pair),
        acc0, acc1, te0, te1, th0, th1, p3,
        scratch_shapes=[pltpu.VMEM((3 * HALF, 512), bf16)],
    )
    tokens = (at, te0, te1, th0, th1)
    r3 = exchange(s3, "z", NZ, 1)
    near, far = call(
        token_parts,
        (shape((2, 192, 2048), f32), shape((2, 192, 2048))),
        blocks, dg, du, tl0, tl1, own, got, p1, p2, p3,
        in_specs=[SM] + [VM] * 9,
        scratch_shapes=[pltpu.VMEM((2 * HALF, 2048), bf16)],
    )
    s2 = call(functools.partial(add_pair, 4), pair, *tokens, r3)
    r2 = exchange(s2, "z", NZ, 0)
    one = shape((1, 3 * HALF, 256))
    mine = exchange(call(neighbour_share, one, *tokens), "z", NZ, 0)
    s1, s0 = call(add_each, (one, one), *tokens, r2)
    r0 = hop_two(s0, -1)
    r1 = exchange(s1, "z", NZ, 1)
    block = call(
        own_block,
        shape((NY, PACK, 128), f32),
        *tokens, mine, r1,
        scratch_shapes=[pltpu.VMEM((1, 3 * HALF, 256), f32)],
    )
    back = call(last_block, shape((NY, PACK, 128)), block, r0)
    sums = call(
        finish_weights,
        (shape((ROWS, 352), f32),) * 3,
        over_y(back), gate_sum, up_sum, down_sum,
    )

    def folded(near, far, body=fold):
        dims = (2, near.shape[1] // 2, 2048)
        return call(body, (shape(dims, f32), shape(dims)), near, far)

    near, far = folded(near, swapped(far, "c"))
    near, far = folded(near, exchange(far, "x", NX, 1), fold_mate)
    near, far = folded(near, swapped(far, "ys"))
    late, early = call(
        finish_tokens,
        (shape((24, 2048)),) * 2,
        near, exchange(far, "x", NX, 0), x_early, cotangent, x_late, gain,
    )
    return (late, early, *sums)


def solution(mesh):
    fine = Mesh(mesh.devices.reshape(NZ, 4, 2, NX, NC), AXES)
    token = P(AXES, None)
    weight = P(("z", "yq", "ys"), ("x", "c"))
    return jax.shard_map(
        on_device,
        mesh=fine,
        in_specs=(token, token, token, P()) + (weight,) * 6,
        out_specs=(token, token) + (weight,) * 3,
        check_vma=False,
    )
```

```python
import functools

import jax
import jax.numpy as jnp
from jax import lax
from jax.experimental import pallas as pl
from jax.experimental.pallas import tpu as pltpu
from jax.sharding import Mesh
from jax.sharding import PartitionSpec as P


eps = 1e-06
f32 = jnp.float32
bf16 = jnp.bfloat16

AXES = ("z", "yq", "ys", "x", "c")
NZ, NY, NX, NC = 8, 8, 4, 2
FLIP = {"z": 0, "x": 1}
ROWS = 32
HALF = 176
MAIN = 128
TAIL = 48
PACK = 136


def call(body, out_shape, *args, mib=16, **kw):
    return pl.pallas_call(
        body,
        out_shape=out_shape,
        compiler_params=pltpu.CompilerParams(vmem_limit_bytes=mib * 1024 * 1024),
        **kw,
    )(*args)


def exchange(x, axis, size, phase):
    pairs = []
    for i in range(size):
        for c in range(NC):
            j = (i + 1) % size if (i + c + phase + FLIP[axis]) % 2 == 0 else (i - 1) % size
            pairs.append((i * NC + c, j * NC + c))
    return lax.ppermute(x, (axis, "c"), pairs)


def hop_two(x, way):
    pairs = []
    for i in range(NZ):
        for c in range(NC):
            j = (i + 2 * way) % NZ if (i + c + FLIP["z"]) % 2 == 0 else (i - 2 * way) % NZ
            pairs.append((i * NC + c, j * NC + c))
    return lax.ppermute(x, ("z", "c"), pairs)


def swapped(x, axis):
    return lax.ppermute(x, axis, [(0, 1), (1, 0)])


def over_y(x):
    return lax.all_to_all(x, ("yq", "ys"), split_axis=0, concat_axis=0, tiled=True)


def dot_tt(left, right):
    return lax.dot_general(left, right, (((1,), (1,)), ((), ())), preferred_element_type=f32)


def dot_nn(left, right):
    return lax.dot_general(left, right, (((1,), (0,)), ((), ())), preferred_element_type=f32)


def pick(*parts):
    out = parts[-1][1]
    lane = lax.broadcasted_iota(jnp.int32, out.shape, out.ndim - 1)
    for bound, part in reversed(parts[:-1]):
        out = jnp.where(lane < bound, part, out)
    return out


def shift(x, by):
    return pltpu.roll(x, by % 128, x.ndim - 1)


def fold_rows(x, start, axis):
    rows = [lax.slice_in_dim(x, 8 * j, 8 * j + 8, axis=axis) for j in range(4)]
    rows = [(16 * j + 16, shift(r, 16 * j - start)) for j, r in enumerate(rows)]
    return pick(*rows, (128, jnp.zeros_like(rows[0][1])))


def unfold_rows(x, axis):
    return jnp.concatenate([shift(x, -16 * j) for j in range(4)], axis=axis)


def normalize(x, gain):
    inv = lax.rsqrt(jnp.mean(x * x, axis=-1, keepdims=True) + eps)
    return inv, x * inv * gain


def prepare(*refs):
    (w_out, t_out), scratch, sem = refs[7:9], refs[9:16], refs[16]
    copies = [pltpu.make_async_copy(a, b, sem.at[i]) for i, (a, b) in enumerate(zip(refs[:7], scratch, strict=True))]
    for copy in copies:
        copy.start()
    for copy in copies[:3]:
        copy.wait()
    weights, (early, cot, late, gain) = scratch[:3], scratch[3:]
    tails = []
    for r in weights:
        tail = r[:, 256:352].astype(f32)
        tails.append(jnp.concatenate([tail, jnp.zeros((ROWS, 32), f32)], axis=1))
    g, u, d = tails
    for h in range(2):
        at = h * TAIL
        tail = pick((48, shift(g, -at)), (96, shift(u, 48 - at)), (128, shift(d, 96 - at)))
        rest = fold_rows(d, at + 32, 0)
        for q in range(4):
            for i, r in enumerate(weights):
                w_out[2 * q + h, ROWS * i : ROWS * (i + 1)] = r[:, h * MAIN : (h + 1) * MAIN]
            w_out[2 * q + h, 96:128] = tail.astype(bf16)
            w_out[2 * q + h, 128:136] = rest.astype(bf16)
    for copy in copies[3:]:
        copy.wait()
    gain = gain[...].astype(f32).reshape(1, 2048)
    t_out[0] = normalize(early[...].astype(f32), gain)[1].astype(bf16)
    t_out[1] = (0.5 * cot[...].astype(f32)).astype(bf16)
    t_out[2] = normalize(late[...].astype(f32), gain)[1].astype(bf16)


def turn_block(r_ref, o_ref):
    tiles = [r_ref[:, 32 * i : 32 * (i + 1)].reshape(NY * ROWS, 128).T for i in range(4)]
    rest = unfold_rows(r_ref[:, 128:136].astype(f32), 1).reshape(NY * ROWS, 128).T
    for i in range(3):
        o_ref[HALF * i : HALF * i + MAIN] = tiles[i]
    tail = tiles[3]
    o_ref[128:176] = tail[0:48]
    o_ref[304:352] = tail[48:96]
    o_ref[480:512] = tail[96:128]
    o_ref[512:528] = rest[0:16].astype(bf16)


def join(a_ref, b_ref, o_ref):
    o_ref[0] = a_ref[...]
    o_ref[1] = b_ref[...]


def turned(f):
    parts = [f[HALF * i : HALF * i + MAIN] for i in range(3)]
    parts.append(jnp.concatenate([f[128:176], f[304:352], f[480:512]], axis=0))
    parts.append(jnp.concatenate([f[512:528], jnp.zeros((112, 256), f.dtype)], axis=0))
    parts = [p.T.reshape(NY, ROWS, 128).astype(f32) for p in parts]
    return jnp.concatenate([*parts[:4], fold_rows(parts[4], 0, 1)], axis=1)


def forward_part(b_ref, ta, tb, own, got, p1, p2, te, th, tl, acc, w):
    for q, piece in enumerate((ta, tb)):
        for n in range(2):
            rows = pl.ds((q * 2 + n) * 48, 48)
            for k in range(8):
                cols = pl.ds(pl.multiple_of(b_ref[k] * 256, 256), 256)
                out = pl.ds(k * 256, 256)
                te[rows, out] = piece[n, 0, :, cols]
                th[rows, out] = piece[n, 1, :, cols]
                tl[rows, out] = piece[n, 2, :, cols]
    for n, block in enumerate((own, got, p1.at[0], p1.at[1], p2.at[0], p2.at[1])):
        w[:, pl.ds(n * 256, 256)] = block[...]
    k = 6 * 256
    g, u, d = w[0:HALF], w[HALF : 2 * HALF], w[2 * HALF : 3 * HALF]
    acc[0] = dot_tt(te[:, :k], g)
    acc[1] = dot_tt(te[:, :k], u)
    acc[2] = dot_tt(th[:, :k], d)


def grad_block(at_ref, te, th, k, o, n, add=None):
    cols = pl.ds(k * 256, 256)
    for rows, t in ((slice(0, 2 * HALF), te), (slice(2 * HALF, 3 * HALF), th)):
        sums = dot_nn(at_ref[0, rows], t[0][:, cols]) + dot_nn(at_ref[1, rows], t[1][:, cols])
        if add is not None:
            sums = sums + add[rows].astype(f32)
        o[n, rows] = sums.astype(o.dtype)


def early_rest(acc0, acc1, te0, te1, th0, th1, p3, dg_ref, du_ref, at_ref, s_ref, w):
    for n in range(2):
        w[:, pl.ds(n * 256, 256)] = p3[n]
    k = 6 * 256
    for h, (acc, te, th) in enumerate(((acc0, te0, th0), (acc1, te1, th1))):
        gate = acc[0] + dot_tt(te[:, k:], w[0:HALF])
        up = acc[1] + dot_tt(te[:, k:], w[HALF : 2 * HALF])
        dh = acc[2] + dot_tt(th[:, k:], w[2 * HALF : 3 * HALF])
        sig = jax.nn.sigmoid(gate)
        silu = gate * sig
        hidden = (silu * up).astype(bf16)
        dg = (dh * up * sig * (1.0 + gate * (1.0 - sig))).astype(bf16)
        du = (dh * silu).astype(bf16)
        dg_ref[h] = dg
        du_ref[h] = du
        at_ref[h, 0:HALF] = dg.T
        at_ref[h, HALF : 2 * HALF] = du.T
        at_ref[h, 2 * HALF : 3 * HALF] = hidden.T
    for n in range(2):
        grad_block(at_ref, (te0, te1), (th0, th1), 6 + n, s_ref, n)


def add_pair(k, at_ref, te0, te1, th0, th1, r_ref, o_ref):
    for n in range(2):
        grad_block(at_ref, (te0, te1), (th0, th1), k + n, o_ref, n, r_ref[n])


def add_each(at_ref, te0, te1, th0, th1, r_ref, o_ref, p_ref):
    for n, o in enumerate((o_ref, p_ref)):
        grad_block(at_ref, (te0, te1), (th0, th1), 2 + n, o, 0, r_ref[n])


def neighbour_share(at_ref, te0, te1, th0, th1, o_ref):
    grad_block(at_ref, (te0, te1), (th0, th1), 1, o_ref, 0)


def own_block(at_ref, te0, te1, th0, th1, q_ref, o_ref, f):
    grad_block(at_ref, (te0, te1), (th0, th1), 0, f, 0, q_ref[0])
    o_ref[...] = turned(f[0])


def last_block(f_ref, r_ref, q_ref, o_ref):
    both = r_ref[0].astype(f32) + q_ref[0].astype(f32)
    o_ref[...] = (f_ref[...] + turned(both)).astype(bf16)


def token_parts(b_ref, dg_ref, du_ref, tl0, tl1, own, got, p1, p2, p3, near, far, w):
    blocks = (own, got) + tuple(p.at[n] for p in (p1, p2, p3) for n in range(2))
    for n, block in enumerate(blocks):
        w[:, pl.ds(n * 256, 256)] = block[0 : 2 * HALF]
    for h, (tl, o) in enumerate(((tl0, near), (tl1, far))):
        gl = dot_tt(tl[...], w[0:HALF])
        ul = dot_tt(tl[...], w[HALF : 2 * HALF])
        hl = (gl * jax.nn.sigmoid(gl) * ul).astype(bf16)
        dg, du = dg_ref[h], du_ref[h]
        for n, block in enumerate(blocks):
            cols = pl.ds(pl.multiple_of(b_ref[n] * 256, 256), 256)
            late = dot_nn(hl, block[2 * HALF : 3 * HALF])
            early = dot_nn(dg, block[0:HALF]) + dot_nn(du, block[HALF : 2 * HALF])
            o[0, :, cols] = late.astype(o.dtype)
            o[1, :, cols] = early.astype(o.dtype)


def fold(n_ref, r_ref, keep, send):
    rows = keep.shape[1]
    for i in range(2):
        keep[i] = n_ref[i, :rows] + r_ref[i, :rows].astype(f32)
        send[i] = (n_ref[i, rows:] + r_ref[i, rows:].astype(f32)).astype(bf16)


def fold_mate(n_ref, r_ref, keep, send):
    for i in range(2):
        sums = n_ref[i] + r_ref[i].astype(f32)
        keep[i] = jnp.concatenate([sums[0:24], sums[48:72]], axis=0)
        send[i] = jnp.concatenate([sums[24:48], sums[72:96]], axis=0).astype(bf16)


def finish_tokens(n_ref, r_ref, e_ref, c_ref, l_ref, g_ref, late, early):
    gain = g_ref[...].astype(f32)
    branch = n_ref[0] + r_ref[0].astype(f32)
    late[...] = (l_ref[...].astype(f32) + 0.5 * branch).astype(bf16)
    d_normed = n_ref[1] + r_ref[1].astype(f32)
    x = e_ref[...].astype(f32)
    inv, _ = normalize(x, gain)
    scaled = d_normed * gain
    d_input = inv * scaled - x * inv**3 * jnp.mean(scaled * x, axis=-1, keepdims=True)
    early[...] = (c_ref[...].astype(f32) + d_input).astype(bf16)


def finish_weights(r_ref, gs, us, ds, go, uo, do):
    total = []
    for h in range(2):
        t = r_ref[h].astype(f32)
        for q in range(1, 4):
            t = t + r_ref[2 * q + h].astype(f32)
        total.append(t)
    t = [t[96:128] for t in total]
    r = [unfold_rows(t[128:136], 0) for t in total]
    g2 = pick((48, t[0]), (128, shift(t[1], 48)))
    u2 = pick((48, shift(t[0], -48)), (128, t[1]))
    d2 = pick((32, shift(t[0], 32)), (48, shift(r[0], 32)), (80, shift(t[1], 80)), (128, shift(r[1], 80)))
    for i, (s, o, t2) in enumerate(((gs, go, g2), (us, uo, u2), (ds, do, d2))):
        for h in range(2):
            cols = slice(h * MAIN, (h + 1) * MAIN)
            o[:, cols] = s[:, cols] + total[h][ROWS * i : ROWS * (i + 1)]
        o[:, 256:352] = s[:, 256:352] + t2[:, :96]


def shape(dims, dtype=bf16):
    return jax.ShapeDtypeStruct(dims, dtype)


VM = pl.BlockSpec(memory_space=pltpu.VMEM)
HB = pl.BlockSpec(memory_space=pltpu.MemorySpace.HBM)
SM = pl.BlockSpec(memory_space=pltpu.SMEM)


def on_device(
    x_late,
    x_early,
    cotangent,
    norm_gain,
    gate_weight,
    up_weight,
    down_weight,
    gate_sum,
    up_sum,
    down_sum,
):
    gain = norm_gain.reshape(1, -1)
    z, c = lax.axis_index("z"), lax.axis_index("c")
    step = 1 - 2 * lax.rem(z + c + FLIP["z"], 2)
    order = jnp.array([0, 1, -1, -2, 2, 3, -3, -4], jnp.int32)
    blocks = lax.rem(z + order * step + 8, 8).astype(jnp.int32)

    given = (gate_weight, up_weight, down_weight, x_early, cotangent, x_late, norm_gain)
    sent, tok = call(
        prepare,
        (shape((NY, PACK, 128)), shape((3, 24, 2048))),
        *(pltpu.with_memory_space_constraint(a, pltpu.HBM) for a in given),
        in_specs=[HB] * 7,
        scratch_shapes=[pltpu.VMEM(a.shape, bf16) for a in given] + [pltpu.SemaphoreType.DMA((7,))],
    )
    own = call(turn_block, shape((3 * HALF, 256)), over_y(sent))
    got = exchange(own, "z", NZ, 0)
    far = hop_two(own, 1)
    p1 = call(join, shape((2, 3 * HALF, 256)), exchange(own, "z", NZ, 1), far)
    p2 = exchange(p1, "z", NZ, 0)
    p3 = exchange(p2, "z", NZ, 1)

    t0 = jnp.concatenate([tok, swapped(tok, "ys")], axis=1)
    ta = call(join, shape((2, 3, 48, 2048)), t0, exchange(t0, "x", NX, 0))
    tb = exchange(ta, "x", NX, 1)
    tc = swapped(ta, "c")
    td = swapped(tb, "c")

    def most(first, second):
        return call(
            forward_part,
            (shape((192, 2048)),) * 3 + (shape((3, 192, HALF), f32),),
            blocks, first, second, own, got, p1, p2,
            in_specs=[SM] + [VM] * 6,
            scratch_shapes=[pltpu.VMEM((3 * HALF, 6 * 256), bf16)],
        )

    te0, th0, tl0, acc0 = most(ta, tb)
    te1, th1, tl1, acc1 = most(tc, td)
    pair = shape((2, 3 * HALF, 256))
    dg, du, at, s3 = call(
        early_rest,
        (shape((2, 192, HALF)), shape((2, 192, HALF)), shape((2, 3 * HALF, 192)), pair),
        acc0, acc1, te0, te1, th0, th1, p3,
        scratch_shapes=[pltpu.VMEM((3 * HALF, 512), bf16)],
    )
    tokens = (at, te0, te1, th0, th1)
    r3 = exchange(s3, "z", NZ, 1)
    near, far = call(
        token_parts,
        (shape((2, 192, 2048), f32), shape((2, 192, 2048))),
        blocks, dg, du, tl0, tl1, own, got, p1, p2, p3,
        in_specs=[SM] + [VM] * 9,
        scratch_shapes=[pltpu.VMEM((2 * HALF, 2048), bf16)],
    )
    s2 = call(functools.partial(add_pair, 4), pair, *tokens, r3)
    r2 = exchange(s2, "z", NZ, 0)
    one = shape((1, 3 * HALF, 256))
    mine = exchange(call(neighbour_share, one, *tokens), "z", NZ, 0)
    s1, s0 = call(add_each, (one, one), *tokens, r2)
    r0 = hop_two(s0, -1)
    r1 = exchange(s1, "z", NZ, 1)
    block = call(
        own_block,
        shape((NY, PACK, 128), f32),
        *tokens, mine,
        scratch_shapes=[pltpu.VMEM((1, 3 * HALF, 256), f32)],
    )
    back = call(last_block, shape((NY, PACK, 128)), block, r0, r1)
    sums = call(
        finish_weights,
        (shape((ROWS, 352), f32),) * 3,
        over_y(back), gate_sum, up_sum, down_sum,
    )

    def folded(near, far, body=fold):
        dims = (2, near.shape[1] // 2, 2048)
        return call(body, (shape(dims, f32), shape(dims)), near, far)

    near, far = folded(near, swapped(far, "c"))
    near, far = folded(near, exchange(far, "x", NX, 1), fold_mate)
    near, far = folded(near, swapped(far, "ys"))
    late, early = call(
        finish_tokens,
        (shape((24, 2048)),) * 2,
        near, exchange(far, "x", NX, 0), x_early, cotangent, x_late, gain,
    )
    return (late, early, *sums)


def solution(mesh):
    fine = Mesh(mesh.devices.reshape(NZ, 4, 2, NX, NC), AXES)
    token = P(AXES, None)
    weight = P(("z", "yq", "ys"), ("x", "c"))
    return jax.shard_map(
        on_device,
        mesh=fine,
        in_specs=(token, token, token, P()) + (weight,) * 6,
        out_specs=(token, token) + (weight,) * 3,
        check_vma=False,
    )
```

```python
import functools

import jax
import jax.numpy as jnp
from jax import lax
from jax.experimental import pallas as pl
from jax.experimental.pallas import tpu as pltpu
from jax.sharding import Mesh
from jax.sharding import PartitionSpec as P


eps = 1e-06
f32 = jnp.float32
bf16 = jnp.bfloat16

AXES = ("z", "yq", "ys", "x", "c")
NZ, NY, NX, NC = 8, 8, 4, 2
FLIP = {"z": 0, "x": 1}
ROWS = 32
HALF = 176
MAIN = 128
TAIL = 48
PACK = 136


def call(body, out_shape, *args, mib=16, **kw):
    return pl.pallas_call(
        body,
        out_shape=out_shape,
        compiler_params=pltpu.CompilerParams(vmem_limit_bytes=mib * 1024 * 1024),
        **kw,
    )(*args)


def exchange(x, axis, size, phase):
    pairs = []
    for i in range(size):
        for c in range(NC):
            j = (i + 1) % size if (i + c + phase + FLIP[axis]) % 2 == 0 else (i - 1) % size
            pairs.append((i * NC + c, j * NC + c))
    return lax.ppermute(x, (axis, "c"), pairs)


def hop_two(x, way):
    pairs = []
    for i in range(NZ):
        for c in range(NC):
            j = (i + 2 * way) % NZ if (i + c + FLIP["z"]) % 2 == 0 else (i - 2 * way) % NZ
            pairs.append((i * NC + c, j * NC + c))
    return lax.ppermute(x, ("z", "c"), pairs)


def swapped(x, axis):
    return lax.ppermute(x, axis, [(0, 1), (1, 0)])


def over_y(x):
    return lax.all_to_all(x, ("yq", "ys"), split_axis=0, concat_axis=0, tiled=True)


def dot_tt(left, right):
    return lax.dot_general(left, right, (((1,), (1,)), ((), ())), preferred_element_type=f32)


def dot_nn(left, right):
    return lax.dot_general(left, right, (((1,), (0,)), ((), ())), preferred_element_type=f32)


def pick(*parts):
    out = parts[-1][1]
    lane = lax.broadcasted_iota(jnp.int32, out.shape, out.ndim - 1)
    for bound, part in reversed(parts[:-1]):
        out = jnp.where(lane < bound, part, out)
    return out


def shift(x, by):
    return pltpu.roll(x, by % 128, x.ndim - 1)


def fold_rows(x, start, axis):
    rows = [lax.slice_in_dim(x, 8 * j, 8 * j + 8, axis=axis) for j in range(4)]
    rows = [(16 * j + 16, shift(r, 16 * j - start)) for j, r in enumerate(rows)]
    return pick(*rows, (128, jnp.zeros_like(rows[0][1])))


def unfold_rows(x, axis):
    return jnp.concatenate([shift(x, -16 * j) for j in range(4)], axis=axis)


def normalize(x, gain):
    inv = lax.rsqrt(jnp.mean(x * x, axis=-1, keepdims=True) + eps)
    return inv, x * inv * gain


def prepare(*refs):
    (w_out, t_out), scratch, sem = refs[7:9], refs[9:16], refs[16]
    copies = [pltpu.make_async_copy(a, b, sem.at[i]) for i, (a, b) in enumerate(zip(refs[:7], scratch, strict=True))]
    for copy in copies:
        copy.start()
    for copy in copies[:3]:
        copy.wait()
    weights, (early, cot, late, gain) = scratch[:3], scratch[3:]
    tails = []
    for r in weights:
        tail = r[:, 256:352].astype(f32)
        tails.append(jnp.concatenate([tail, jnp.zeros((ROWS, 32), f32)], axis=1))
    g, u, d = tails
    for h in range(2):
        at = h * TAIL
        tail = pick((48, shift(g, -at)), (96, shift(u, 48 - at)), (128, shift(d, 96 - at)))
        rest = fold_rows(d, at + 32, 0)
        for q in range(4):
            for i, r in enumerate(weights):
                w_out[2 * q + h, ROWS * i : ROWS * (i + 1)] = r[:, h * MAIN : (h + 1) * MAIN]
            w_out[2 * q + h, 96:128] = tail.astype(bf16)
            w_out[2 * q + h, 128:136] = rest.astype(bf16)
    for copy in copies[3:]:
        copy.wait()
    gain = gain[...].astype(f32).reshape(1, 2048)
    t_out[0] = normalize(early[...].astype(f32), gain)[1].astype(bf16)
    t_out[1] = (0.5 * cot[...].astype(f32)).astype(bf16)
    t_out[2] = normalize(late[...].astype(f32), gain)[1].astype(bf16)


def turn_block(r_ref, o_ref):
    tiles = [r_ref[:, 32 * i : 32 * (i + 1)].reshape(NY * ROWS, 128).T for i in range(4)]
    rest = unfold_rows(r_ref[:, 128:136].astype(f32), 1).reshape(NY * ROWS, 128).T
    for i in range(3):
        o_ref[HALF * i : HALF * i + MAIN] = tiles[i]
    tail = tiles[3]
    o_ref[128:176] = tail[0:48]
    o_ref[304:352] = tail[48:96]
    o_ref[480:512] = tail[96:128]
    o_ref[512:528] = rest[0:16].astype(bf16)


def join(a_ref, b_ref, o_ref):
    o_ref[0] = a_ref[...]
    o_ref[1] = b_ref[...]


def turned(f):
    parts = [f[HALF * i : HALF * i + MAIN] for i in range(3)]
    parts.append(jnp.concatenate([f[128:176], f[304:352], f[480:512]], axis=0))
    parts.append(jnp.concatenate([f[512:528], jnp.zeros((112, 256), f.dtype)], axis=0))
    parts = [p.T.reshape(NY, ROWS, 128).astype(f32) for p in parts]
    return jnp.concatenate([*parts[:4], fold_rows(parts[4], 0, 1)], axis=1)


def forward_part(b_ref, ta, tb, own, got, p1, p2, te, th, tl, acc, w):
    for q, piece in enumerate((ta, tb)):
        for n in range(2):
            rows = pl.ds((q * 2 + n) * 48, 48)
            for k in range(8):
                cols = pl.ds(pl.multiple_of(b_ref[k] * 256, 256), 256)
                out = pl.ds(k * 256, 256)
                te[rows, out] = piece[n, 0, :, cols]
                th[rows, out] = piece[n, 1, :, cols]
                tl[rows, out] = piece[n, 2, :, cols]
    for n, block in enumerate((own, got, p1.at[0], p1.at[1], p2.at[0], p2.at[1])):
        w[:, pl.ds(n * 256, 256)] = block[...]
    k = 6 * 256
    g, u, d = w[0:HALF], w[HALF : 2 * HALF], w[2 * HALF : 3 * HALF]
    acc[0] = dot_tt(te[:, :k], g)
    acc[1] = dot_tt(te[:, :k], u)
    acc[2] = dot_tt(th[:, :k], d)


def grad_block(at_ref, te, th, k, o, n, add=None):
    cols = pl.ds(k * 256, 256)
    for rows, t in ((slice(0, 2 * HALF), te), (slice(2 * HALF, 3 * HALF), th)):
        sums = dot_nn(at_ref[0, rows], t[0][:, cols]) + dot_nn(at_ref[1, rows], t[1][:, cols])
        if add is not None:
            sums = sums + add[rows].astype(f32)
        o[n, rows] = sums.astype(o.dtype)


def early_rest(acc0, acc1, te0, te1, th0, th1, p3, dg_ref, du_ref, at_ref, s_ref, w):
    for n in range(2):
        w[:, pl.ds(n * 256, 256)] = p3[n]
    k = 6 * 256
    for h, (acc, te, th) in enumerate(((acc0, te0, th0), (acc1, te1, th1))):
        gate = acc[0] + dot_tt(te[:, k:], w[0:HALF])
        up = acc[1] + dot_tt(te[:, k:], w[HALF : 2 * HALF])
        dh = acc[2] + dot_tt(th[:, k:], w[2 * HALF : 3 * HALF])
        sig = jax.nn.sigmoid(gate)
        silu = gate * sig
        hidden = (silu * up).astype(bf16)
        dg = (dh * up * sig * (1.0 + gate * (1.0 - sig))).astype(bf16)
        du = (dh * silu).astype(bf16)
        dg_ref[h] = dg
        du_ref[h] = du
        at_ref[h, 0:HALF] = dg.T
        at_ref[h, HALF : 2 * HALF] = du.T
        at_ref[h, 2 * HALF : 3 * HALF] = hidden.T
    for n in range(2):
        grad_block(at_ref, (te0, te1), (th0, th1), 6 + n, s_ref, n)


def shares(k, at_ref, te0, te1, th0, th1, o_ref):
    for n in range(2):
        grad_block(at_ref, (te0, te1), (th0, th1), k + n, o_ref, n)


def add_pair(f_ref, r_ref, o_ref):
    o_ref[...] = (f_ref[...] + r_ref[...].astype(f32)).astype(bf16)


def add_each(f_ref, r_ref, o_ref, p_ref):
    for n, o in enumerate((o_ref, p_ref)):
        o[0] = (f_ref[n] + r_ref[n].astype(f32)).astype(bf16)


def neighbour_share(at_ref, te0, te1, th0, th1, o_ref):
    grad_block(at_ref, (te0, te1), (th0, th1), 1, o_ref, 0)


def own_block(at_ref, te0, te1, th0, th1, q_ref, o_ref, f):
    grad_block(at_ref, (te0, te1), (th0, th1), 0, f, 0, q_ref[0])
    o_ref[...] = turned(f[0])


def last_block(f_ref, r_ref, o_ref):
    o_ref[...] = (f_ref[...] + turned(r_ref[0])).astype(o_ref.dtype)


def token_parts(b_ref, dg_ref, du_ref, tl0, tl1, own, got, p1, p2, p3, near, far, w):
    blocks = (own, got) + tuple(p.at[n] for p in (p1, p2, p3) for n in range(2))
    for n, block in enumerate(blocks):
        w[:, pl.ds(n * 256, 256)] = block[0 : 2 * HALF]
    for h, (tl, o) in enumerate(((tl0, near), (tl1, far))):
        gl = dot_tt(tl[...], w[0:HALF])
        ul = dot_tt(tl[...], w[HALF : 2 * HALF])
        hl = (gl * jax.nn.sigmoid(gl) * ul).astype(bf16)
        dg, du = dg_ref[h], du_ref[h]
        for n, block in enumerate(blocks):
            cols = pl.ds(pl.multiple_of(b_ref[n] * 256, 256), 256)
            late = dot_nn(hl, block[2 * HALF : 3 * HALF])
            early = dot_nn(dg, block[0:HALF]) + dot_nn(du, block[HALF : 2 * HALF])
            o[0, :, cols] = late.astype(o.dtype)
            o[1, :, cols] = early.astype(o.dtype)


def fold(n_ref, r_ref, keep, send):
    rows = keep.shape[1]
    for i in range(2):
        keep[i] = n_ref[i, :rows] + r_ref[i, :rows].astype(f32)
        send[i] = (n_ref[i, rows:] + r_ref[i, rows:].astype(f32)).astype(bf16)


def fold_mate(n_ref, r_ref, keep, send):
    for i in range(2):
        sums = n_ref[i] + r_ref[i].astype(f32)
        keep[i] = jnp.concatenate([sums[0:24], sums[48:72]], axis=0)
        send[i] = jnp.concatenate([sums[24:48], sums[72:96]], axis=0).astype(bf16)


def finish_tokens(n_ref, r_ref, e_ref, c_ref, l_ref, g_ref, late, early):
    gain = g_ref[...].astype(f32)
    branch = n_ref[0] + r_ref[0].astype(f32)
    late[...] = (l_ref[...].astype(f32) + 0.5 * branch).astype(bf16)
    d_normed = n_ref[1] + r_ref[1].astype(f32)
    x = e_ref[...].astype(f32)
    inv, _ = normalize(x, gain)
    scaled = d_normed * gain
    d_input = inv * scaled - x * inv**3 * jnp.mean(scaled * x, axis=-1, keepdims=True)
    early[...] = (c_ref[...].astype(f32) + d_input).astype(bf16)


def finish_weights(r_ref, gs, us, ds, go, uo, do):
    total = []
    for h in range(2):
        t = r_ref[h].astype(f32)
        for q in range(1, 4):
            t = t + r_ref[2 * q + h].astype(f32)
        total.append(t)
    t = [t[96:128] for t in total]
    r = [unfold_rows(t[128:136], 0) for t in total]
    g2 = pick((48, t[0]), (128, shift(t[1], 48)))
    u2 = pick((48, shift(t[0], -48)), (128, t[1]))
    d2 = pick((32, shift(t[0], 32)), (48, shift(r[0], 32)), (80, shift(t[1], 80)), (128, shift(r[1], 80)))
    for i, (s, o, t2) in enumerate(((gs, go, g2), (us, uo, u2), (ds, do, d2))):
        for h in range(2):
            cols = slice(h * MAIN, (h + 1) * MAIN)
            o[:, cols] = s[:, cols] + total[h][ROWS * i : ROWS * (i + 1)]
        o[:, 256:352] = s[:, 256:352] + t2[:, :96]


def shape(dims, dtype=bf16):
    return jax.ShapeDtypeStruct(dims, dtype)


VM = pl.BlockSpec(memory_space=pltpu.VMEM)
HB = pl.BlockSpec(memory_space=pltpu.MemorySpace.HBM)
SM = pl.BlockSpec(memory_space=pltpu.SMEM)


def on_device(
    x_late,
    x_early,
    cotangent,
    norm_gain,
    gate_weight,
    up_weight,
    down_weight,
    gate_sum,
    up_sum,
    down_sum,
):
    gain = norm_gain.reshape(1, -1)
    z, c = lax.axis_index("z"), lax.axis_index("c")
    step = 1 - 2 * lax.rem(z + c + FLIP["z"], 2)
    order = jnp.array([0, 1, -1, -2, 2, 3, -3, -4], jnp.int32)
    blocks = lax.rem(z + order * step + 8, 8).astype(jnp.int32)

    given = (gate_weight, up_weight, down_weight, x_early, cotangent, x_late, norm_gain)
    sent, tok = call(
        prepare,
        (shape((NY, PACK, 128)), shape((3, 24, 2048))),
        *(pltpu.with_memory_space_constraint(a, pltpu.HBM) for a in given),
        in_specs=[HB] * 7,
        scratch_shapes=[pltpu.VMEM(a.shape, bf16) for a in given] + [pltpu.SemaphoreType.DMA((7,))],
    )
    own = call(turn_block, shape((3 * HALF, 256)), over_y(sent))
    got = exchange(own, "z", NZ, 0)
    far = hop_two(own, 1)
    p1 = call(join, shape((2, 3 * HALF, 256)), exchange(own, "z", NZ, 1), far)
    p2 = exchange(p1, "z", NZ, 0)
    p3 = exchange(p2, "z", NZ, 1)

    t0 = jnp.concatenate([tok, swapped(tok, "ys")], axis=1)
    ta = call(join, shape((2, 3, 48, 2048)), t0, exchange(t0, "x", NX, 0))
    tb = exchange(ta, "x", NX, 1)
    tc = swapped(ta, "c")
    td = swapped(tb, "c")

    def most(first, second):
        return call(
            forward_part,
            (shape((192, 2048)),) * 3 + (shape((3, 192, HALF), f32),),
            blocks, first, second, own, got, p1, p2,
            in_specs=[SM] + [VM] * 6,
            scratch_shapes=[pltpu.VMEM((3 * HALF, 6 * 256), bf16)],
        )

    te0, th0, tl0, acc0 = most(ta, tb)
    te1, th1, tl1, acc1 = most(tc, td)
    pair = shape((2, 3 * HALF, 256))
    dg, du, at, s3 = call(
        early_rest,
        (shape((2, 192, HALF)), shape((2, 192, HALF)), shape((2, 3 * HALF, 192)), pair),
        acc0, acc1, te0, te1, th0, th1, p3,
        scratch_shapes=[pltpu.VMEM((3 * HALF, 512), bf16)],
    )
    tokens = (at, te0, te1, th0, th1)
    r3 = exchange(s3, "z", NZ, 1)
    near, far = call(
        token_parts,
        (shape((2, 192, 2048), f32), shape((2, 192, 2048))),
        blocks, dg, du, tl0, tl1, own, got, p1, p2, p3,
        in_specs=[SM] + [VM] * 9,
        scratch_shapes=[pltpu.VMEM((2 * HALF, 2048), bf16)],
    )
    both = shape((2, 3 * HALF, 256), f32)
    s2 = call(add_pair, pair, call(functools.partial(shares, 4), both, *tokens), r3)
    r2 = exchange(s2, "z", NZ, 0)
    one = shape((1, 3 * HALF, 256))
    mine = exchange(call(neighbour_share, one, *tokens), "z", NZ, 0)
    pre = call(functools.partial(shares, 2), both, *tokens)
    s1, s0 = call(add_each, (one, one), pre, r2)
    r0 = hop_two(s0, -1)
    r1 = exchange(s1, "z", NZ, 1)
    block = call(
        own_block,
        shape((NY, PACK, 128), f32),
        *tokens, mine,
        scratch_shapes=[pltpu.VMEM((1, 3 * HALF, 256), f32)],
    )
    block = call(last_block, shape((NY, PACK, 128), f32), block, r0)
    back = call(last_block, shape((NY, PACK, 128)), block, r1)
    sums = call(
        finish_weights,
        (shape((ROWS, 352), f32),) * 3,
        over_y(back), gate_sum, up_sum, down_sum,
    )

    def folded(near, far, body=fold):
        dims = (2, near.shape[1] // 2, 2048)
        return call(body, (shape(dims, f32), shape(dims)), near, far)

    near, far = folded(near, swapped(far, "c"))
    near, far = folded(near, exchange(far, "x", NX, 1), fold_mate)
    near, far = folded(near, swapped(far, "ys"))
    late, early = call(
        finish_tokens,
        (shape((24, 2048)),) * 2,
        near, exchange(far, "x", NX, 0), x_early, cotangent, x_late, gain,
    )
    return (late, early, *sums)


def solution(mesh):
    fine = Mesh(mesh.devices.reshape(NZ, 4, 2, NX, NC), AXES)
    token = P(AXES, None)
    weight = P(("z", "yq", "ys"), ("x", "c"))
    return jax.shard_map(
        on_device,
        mesh=fine,
        in_specs=(token, token, token, P()) + (weight,) * 6,
        out_specs=(token, token) + (weight,) * 3,
        check_vma=False,
    )
```

```python
import functools

import jax
import jax.numpy as jnp
from jax import lax
from jax.experimental import pallas as pl
from jax.experimental.pallas import tpu as pltpu
from jax.sharding import Mesh
from jax.sharding import PartitionSpec as P


eps = 1e-06
f32 = jnp.float32
bf16 = jnp.bfloat16

AXES = ("z", "yq", "ys", "x", "c")
NZ, NY, NX, NC = 8, 8, 4, 2
FLIP = {"z": 0, "x": 1}
ROWS = 32
HALF = 176
MAIN = 128
TAIL = 48
PACK = 136


def call(body, out_shape, *args, mib=16, **kw):
    return pl.pallas_call(
        body,
        out_shape=out_shape,
        compiler_params=pltpu.CompilerParams(vmem_limit_bytes=mib * 1024 * 1024),
        **kw,
    )(*args)


def exchange(x, axis, size, phase):
    pairs = []
    for i in range(size):
        for c in range(NC):
            j = (i + 1) % size if (i + c + phase + FLIP[axis]) % 2 == 0 else (i - 1) % size
            pairs.append((i * NC + c, j * NC + c))
    return lax.ppermute(x, (axis, "c"), pairs)


def hop_two(x, way):
    pairs = []
    for i in range(NZ):
        for c in range(NC):
            j = (i + 2 * way) % NZ if (i + c + FLIP["z"]) % 2 == 0 else (i - 2 * way) % NZ
            pairs.append((i * NC + c, j * NC + c))
    return lax.ppermute(x, ("z", "c"), pairs)


def swapped(x, axis):
    return lax.ppermute(x, axis, [(0, 1), (1, 0)])


def over_y(x):
    return lax.all_to_all(x, ("yq", "ys"), split_axis=0, concat_axis=0, tiled=True)


def dot_tt(left, right):
    return lax.dot_general(left, right, (((1,), (1,)), ((), ())), preferred_element_type=f32)


def dot_nn(left, right):
    return lax.dot_general(left, right, (((1,), (0,)), ((), ())), preferred_element_type=f32)


def pick(*parts):
    out = parts[-1][1]
    lane = lax.broadcasted_iota(jnp.int32, out.shape, out.ndim - 1)
    for bound, part in reversed(parts[:-1]):
        out = jnp.where(lane < bound, part, out)
    return out


def shift(x, by):
    return pltpu.roll(x, by % 128, x.ndim - 1)


def fold_rows(x, start, axis):
    rows = [lax.slice_in_dim(x, 8 * j, 8 * j + 8, axis=axis) for j in range(4)]
    rows = [(16 * j + 16, shift(r, 16 * j - start)) for j, r in enumerate(rows)]
    return pick(*rows, (128, jnp.zeros_like(rows[0][1])))


def unfold_rows(x, axis):
    return jnp.concatenate([shift(x, -16 * j) for j in range(4)], axis=axis)


def normalize(x, gain):
    inv = lax.rsqrt(jnp.mean(x * x, axis=-1, keepdims=True) + eps)
    return inv, x * inv * gain


def prepare(*refs):
    (w_out, t_out), scratch, sem = refs[7:9], refs[9:16], refs[16]
    copies = [pltpu.make_async_copy(a, b, sem.at[i]) for i, (a, b) in enumerate(zip(refs[:7], scratch, strict=True))]
    for copy in copies:
        copy.start()
    for copy in copies[:3]:
        copy.wait()
    weights, (early, cot, late, gain) = scratch[:3], scratch[3:]
    tails = []
    for r in weights:
        tail = r[:, 256:352].astype(f32)
        tails.append(jnp.concatenate([tail, jnp.zeros((ROWS, 32), f32)], axis=1))
    g, u, d = tails
    for h in range(2):
        at = h * TAIL
        tail = pick((48, shift(g, -at)), (96, shift(u, 48 - at)), (128, shift(d, 96 - at)))
        rest = fold_rows(d, at + 32, 0)
        for q in range(4):
            for i, r in enumerate(weights):
                w_out[2 * q + h, ROWS * i : ROWS * (i + 1)] = r[:, h * MAIN : (h + 1) * MAIN]
            w_out[2 * q + h, 96:128] = tail.astype(bf16)
            w_out[2 * q + h, 128:136] = rest.astype(bf16)
    for copy in copies[3:]:
        copy.wait()
    gain = gain[...].astype(f32).reshape(1, 2048)
    t_out[0] = normalize(early[...].astype(f32), gain)[1].astype(bf16)
    t_out[1] = (0.5 * cot[...].astype(f32)).astype(bf16)
    t_out[2] = normalize(late[...].astype(f32), gain)[1].astype(bf16)


def turn_block(r_ref, o_ref):
    tiles = [r_ref[:, 32 * i : 32 * (i + 1)].reshape(NY * ROWS, 128).T for i in range(4)]
    rest = unfold_rows(r_ref[:, 128:136].astype(f32), 1).astype(bf16).reshape(NY * ROWS, 128).T
    for i in range(3):
        o_ref[HALF * i : HALF * i + MAIN] = tiles[i]
    tail = tiles[3]
    o_ref[128:176] = tail[0:48]
    o_ref[304:352] = tail[48:96]
    o_ref[480:512] = tail[96:128]
    o_ref[512:528] = rest[0:16]


def join(a_ref, b_ref, o_ref):
    o_ref[0] = a_ref[...]
    o_ref[1] = b_ref[...]


def turned(f):
    parts = [f[HALF * i : HALF * i + MAIN] for i in range(3)]
    parts.append(jnp.concatenate([f[128:176], f[304:352], f[480:512]], axis=0))
    few = f[512:528].T.astype(f32)
    parts = [p.T.reshape(NY, ROWS, 128).astype(f32) for p in parts]
    few = jnp.concatenate([few, jnp.zeros((256, 112), f32)], axis=1)
    parts.append(few.reshape(NY, ROWS, 128))
    return jnp.concatenate([*parts[:4], fold_rows(parts[4], 0, 1)], axis=1)


def forward_part(b_ref, ta, tb, own, got, p1, p2, te, th, tl, acc, w):
    for q, piece in enumerate((ta, tb)):
        for n in range(2):
            rows = pl.ds((q * 2 + n) * 48, 48)
            for k in range(8):
                cols = pl.ds(pl.multiple_of(b_ref[k] * 256, 256), 256)
                out = pl.ds(k * 256, 256)
                te[rows, out] = piece[n, 0, :, cols]
                th[rows, out] = piece[n, 1, :, cols]
                tl[rows, out] = piece[n, 2, :, cols]
    for n, block in enumerate((own, got, p1.at[0], p1.at[1], p2.at[0], p2.at[1])):
        w[:, pl.ds(n * 256, 256)] = block[...]
    k = 6 * 256
    g, u, d = w[0:HALF], w[HALF : 2 * HALF], w[2 * HALF : 3 * HALF]
    acc[0] = dot_tt(te[:, :k], g)
    acc[1] = dot_tt(te[:, :k], u)
    acc[2] = dot_tt(th[:, :k], d)


def grad_block(at_ref, te, th, k, o, n, add=None):
    cols = pl.ds(k * 256, 256)
    for rows, t in ((slice(0, 2 * HALF), te), (slice(2 * HALF, 3 * HALF), th)):
        sums = dot_nn(at_ref[0, rows], t[0][:, cols]) + dot_nn(at_ref[1, rows], t[1][:, cols])
        if add is not None:
            sums = sums + add[rows].astype(f32)
        o[n, rows] = sums.astype(o.dtype)


def early_rest(acc0, acc1, te0, te1, th0, th1, p3, dg_ref, du_ref, at_ref, s_ref, w):
    for n in range(2):
        w[:, pl.ds(n * 256, 256)] = p3[n]
    k = 6 * 256
    for h, (acc, te, th) in enumerate(((acc0, te0, th0), (acc1, te1, th1))):
        gate = acc[0] + dot_tt(te[:, k:], w[0:HALF])
        up = acc[1] + dot_tt(te[:, k:], w[HALF : 2 * HALF])
        dh = acc[2] + dot_tt(th[:, k:], w[2 * HALF : 3 * HALF])
        sig = jax.nn.sigmoid(gate)
        silu = gate * sig
        hidden = (silu * up).astype(bf16)
        dg = (dh * up * sig * (1.0 + gate * (1.0 - sig))).astype(bf16)
        du = (dh * silu).astype(bf16)
        dg_ref[h] = dg
        du_ref[h] = du
        at_ref[h, 0:HALF] = dg.T
        at_ref[h, HALF : 2 * HALF] = du.T
        at_ref[h, 2 * HALF : 3 * HALF] = hidden.T
    for n in range(2):
        grad_block(at_ref, (te0, te1), (th0, th1), 6 + n, s_ref, n)


def shares(k, at_ref, te0, te1, th0, th1, o_ref):
    for n in range(2):
        grad_block(at_ref, (te0, te1), (th0, th1), k + n, o_ref, n)


def add_pair(f_ref, r_ref, o_ref):
    o_ref[...] = (f_ref[...] + r_ref[...].astype(f32)).astype(bf16)


def add_each(f_ref, r_ref, o_ref, p_ref):
    for n, o in enumerate((o_ref, p_ref)):
        o[0] = (f_ref[n] + r_ref[n].astype(f32)).astype(bf16)


def neighbour_share(at_ref, te0, te1, th0, th1, o_ref):
    grad_block(at_ref, (te0, te1), (th0, th1), 1, o_ref, 0)


def own_block(at_ref, te0, te1, th0, th1, q_ref, o_ref, f):
    grad_block(at_ref, (te0, te1), (th0, th1), 0, f, 0, q_ref[0])
    o_ref[...] = turned(f[0])


def last_block(f_ref, r_ref, o_ref):
    o_ref[...] = (f_ref[...] + turned(r_ref[0])).astype(o_ref.dtype)


def token_parts(b_ref, dg_ref, du_ref, tl0, tl1, own, got, p1, p2, p3, near, far, w):
    blocks = (own, got) + tuple(p.at[n] for p in (p1, p2, p3) for n in range(2))
    for n, block in enumerate(blocks):
        w[:, pl.ds(n * 256, 256)] = block[0 : 2 * HALF]
    for h, (tl, o) in enumerate(((tl0, near), (tl1, far))):
        gl = dot_tt(tl[...], w[0:HALF])
        ul = dot_tt(tl[...], w[HALF : 2 * HALF])
        hl = (gl * jax.nn.sigmoid(gl) * ul).astype(bf16)
        dg, du = dg_ref[h], du_ref[h]
        for n, block in enumerate(blocks):
            cols = pl.ds(pl.multiple_of(b_ref[n] * 256, 256), 256)
            late = dot_nn(hl, block[2 * HALF : 3 * HALF])
            early = dot_nn(dg, block[0:HALF]) + dot_nn(du, block[HALF : 2 * HALF])
            o[0, :, cols] = late.astype(o.dtype)
            o[1, :, cols] = early.astype(o.dtype)


def fold(n_ref, r_ref, keep, send):
    rows = keep.shape[1]
    for i in range(2):
        keep[i] = n_ref[i, :rows] + r_ref[i, :rows].astype(f32)
        send[i] = (n_ref[i, rows:] + r_ref[i, rows:].astype(f32)).astype(bf16)


def fold_mate(n_ref, r_ref, keep, send):
    for i in range(2):
        sums = n_ref[i] + r_ref[i].astype(f32)
        keep[i] = jnp.concatenate([sums[0:24], sums[48:72]], axis=0)
        send[i] = jnp.concatenate([sums[24:48], sums[72:96]], axis=0).astype(bf16)


def finish_tokens(n_ref, r_ref, e_ref, c_ref, l_ref, g_ref, late, early):
    gain = g_ref[...].astype(f32)
    branch = n_ref[0] + r_ref[0].astype(f32)
    late[...] = (l_ref[...].astype(f32) + 0.5 * branch).astype(bf16)
    d_normed = n_ref[1] + r_ref[1].astype(f32)
    x = e_ref[...].astype(f32)
    inv, _ = normalize(x, gain)
    scaled = d_normed * gain
    d_input = inv * scaled - x * inv**3 * jnp.mean(scaled * x, axis=-1, keepdims=True)
    early[...] = (c_ref[...].astype(f32) + d_input).astype(bf16)


def finish_weights(r_ref, gs, us, ds, go, uo, do):
    total = []
    for h in range(2):
        t = r_ref[h].astype(f32)
        for q in range(1, 4):
            t = t + r_ref[2 * q + h].astype(f32)
        total.append(t)
    t = [t[96:128] for t in total]
    r = [unfold_rows(t[128:136], 0) for t in total]
    g2 = pick((48, t[0]), (128, shift(t[1], 48)))
    u2 = pick((48, shift(t[0], -48)), (128, t[1]))
    d2 = pick((32, shift(t[0], 32)), (48, shift(r[0], 32)), (80, shift(t[1], 80)), (128, shift(r[1], 80)))
    for i, (s, o, t2) in enumerate(((gs, go, g2), (us, uo, u2), (ds, do, d2))):
        for h in range(2):
            cols = slice(h * MAIN, (h + 1) * MAIN)
            o[:, cols] = s[:, cols] + total[h][ROWS * i : ROWS * (i + 1)]
        o[:, 256:352] = s[:, 256:352] + t2[:, :96]


def shape(dims, dtype=bf16):
    return jax.ShapeDtypeStruct(dims, dtype)


VM = pl.BlockSpec(memory_space=pltpu.VMEM)
HB = pl.BlockSpec(memory_space=pltpu.MemorySpace.HBM)
SM = pl.BlockSpec(memory_space=pltpu.SMEM)


def on_device(
    x_late,
    x_early,
    cotangent,
    norm_gain,
    gate_weight,
    up_weight,
    down_weight,
    gate_sum,
    up_sum,
    down_sum,
):
    gain = norm_gain.reshape(1, -1)
    z, c = lax.axis_index("z"), lax.axis_index("c")
    step = 1 - 2 * lax.rem(z + c + FLIP["z"], 2)
    order = jnp.array([0, 1, -1, -2, 2, 3, -3, -4], jnp.int32)
    blocks = lax.rem(z + order * step + 8, 8).astype(jnp.int32)

    given = (gate_weight, up_weight, down_weight, x_early, cotangent, x_late, norm_gain)
    sent, tok = call(
        prepare,
        (shape((NY, PACK, 128)), shape((3, 24, 2048))),
        *(pltpu.with_memory_space_constraint(a, pltpu.HBM) for a in given),
        in_specs=[HB] * 7,
        scratch_shapes=[pltpu.VMEM(a.shape, bf16) for a in given] + [pltpu.SemaphoreType.DMA((7,))],
    )
    own = call(turn_block, shape((3 * HALF, 256)), over_y(sent))
    got = exchange(own, "z", NZ, 0)
    far = hop_two(own, 1)
    p1 = call(join, shape((2, 3 * HALF, 256)), exchange(own, "z", NZ, 1), far)
    p2 = exchange(p1, "z", NZ, 0)
    p3 = exchange(p2, "z", NZ, 1)

    t0 = jnp.concatenate([tok, swapped(tok, "ys")], axis=1)
    ta = call(join, shape((2, 3, 48, 2048)), t0, exchange(t0, "x", NX, 0))
    tb = exchange(ta, "x", NX, 1)
    tc = swapped(ta, "c")
    td = swapped(tb, "c")

    def most(first, second):
        return call(
            forward_part,
            (shape((192, 2048)),) * 3 + (shape((3, 192, HALF), f32),),
            blocks, first, second, own, got, p1, p2,
            in_specs=[SM] + [VM] * 6,
            scratch_shapes=[pltpu.VMEM((3 * HALF, 6 * 256), bf16)],
        )

    te0, th0, tl0, acc0 = most(ta, tb)
    te1, th1, tl1, acc1 = most(tc, td)
    pair = shape((2, 3 * HALF, 256))
    dg, du, at, s3 = call(
        early_rest,
        (shape((2, 192, HALF)), shape((2, 192, HALF)), shape((2, 3 * HALF, 192)), pair),
        acc0, acc1, te0, te1, th0, th1, p3,
        scratch_shapes=[pltpu.VMEM((3 * HALF, 512), bf16)],
    )
    tokens = (at, te0, te1, th0, th1)
    r3 = exchange(s3, "z", NZ, 1)
    near, far = call(
        token_parts,
        (shape((2, 192, 2048), f32), shape((2, 192, 2048))),
        blocks, dg, du, tl0, tl1, own, got, p1, p2, p3,
        in_specs=[SM] + [VM] * 9,
        scratch_shapes=[pltpu.VMEM((2 * HALF, 2048), bf16)],
    )
    both = shape((2, 3 * HALF, 256), f32)
    s2 = call(add_pair, pair, call(functools.partial(shares, 4), both, *tokens), r3)
    r2 = exchange(s2, "z", NZ, 0)
    one = shape((1, 3 * HALF, 256))
    mine = exchange(call(neighbour_share, one, *tokens), "z", NZ, 0)
    pre = call(functools.partial(shares, 2), both, *tokens)
    s1, s0 = call(add_each, (one, one), pre, r2)
    r0 = hop_two(s0, -1)
    r1 = exchange(s1, "z", NZ, 1)
    block = call(
        own_block,
        shape((NY, PACK, 128), f32),
        *tokens, mine,
        scratch_shapes=[pltpu.VMEM((1, 3 * HALF, 256), f32)],
    )
    block = call(last_block, shape((NY, PACK, 128), f32), block, r0)
    back = call(last_block, shape((NY, PACK, 128)), block, r1)
    sums = call(
        finish_weights,
        (shape((ROWS, 352), f32),) * 3,
        over_y(back), gate_sum, up_sum, down_sum,
    )

    def folded(near, far, body=fold):
        dims = (2, near.shape[1] // 2, 2048)
        return call(body, (shape(dims, f32), shape(dims)), near, far)

    near, far = folded(near, swapped(far, "c"))
    near, far = folded(near, exchange(far, "x", NX, 1), fold_mate)
    near, far = folded(near, swapped(far, "ys"))
    late, early = call(
        finish_tokens,
        (shape((24, 2048)),) * 2,
        near, exchange(far, "x", NX, 0), x_early, cotangent, x_late, gain,
    )
    return (late, early, *sums)


def solution(mesh):
    fine = Mesh(mesh.devices.reshape(NZ, 4, 2, NX, NC), AXES)
    token = P(AXES, None)
    weight = P(("z", "yq", "ys"), ("x", "c"))
    return jax.shard_map(
        on_device,
        mesh=fine,
        in_specs=(token, token, token, P()) + (weight,) * 6,
        out_specs=(token, token) + (weight,) * 3,
        check_vma=False,
    )
```
